32 devices in a mesh: kv: 16 (over z, y, core), tp: 2 (over x).
Axes of the slice: x: 2, y: 2, z: 4, core: 2. Of those that a mesh axis runs over, the one named last changes fastest.
Arguments:
- queries: bfloat16 [4096, 1536], P('kv', 'tp'), may hold values from -6 to 6
- keys: bfloat16 [4096, 256], P('kv', 'tp'), may hold values from -6 to 6
- values: bfloat16 [4096, 256], P('kv', 'tp'), may hold values from -6 to 6
- log_sums: float32 [12, 4096], P('tp', 'kv'), may hold values from 6 to 7.5
- out_grad: bfloat16 [4096, 1536], P('kv', 'tp'), may hold values from -6 to 6
- chosen: int32 [64, 2, 8], P('kv', 'tp'), may hold values from 0 to 63, as said below
- inputs: bfloat16 [4096, 3072], P('kv', 'tp'), may hold values from -6 to 6
Outputs:
- query_grad: bfloat16 [4096, 1536], P('kv', 'tp')
- key_grad: bfloat16 [4096, 256], P('kv', 'tp')
- value_grad: bfloat16 [4096, 256], P('kv', 'tp')
- weight_grad: float32 [3072, 256], P('kv', 'tp')
The draws below stay inside these ranges and needn't reach their ends.
Inputs may be any that keep to these rules, and one draw needn't show every extreme that they name: `chosen`: for query block g and key head h, every slot holds g (an empty slot) or a key block c with g - 16 <= c < g; the blocks of the live slots of one list are distinct; each list has between 4 and 8 live slots, except that query block g has at most g of them (block 0 has none).
All inputs are finite; a program needn't handle non-finite values.
Results may differ from the reference program's by a relative error of at most 0.0049.
Values may be sent and summed in bfloat16 or wider, within the bound.
A program may use at most 64 MiB of HBM per device.

```python
import jax
import jax.numpy as jnp
from jax import lax

D = 3072
HDIM = 128
QPK = 6
BLK = 64
SEL = 8
REACH = 4
BPD = 4
KVH = 2
HEADS = 12
NBLK = 64
TOKENS = 4096


def draw_chosen(key, part):
    window_span = REACH * BPD
    order_key = jax.random.fold_in(key, 11)
    count_key = jax.random.fold_in(key, 12)
    blocks = jnp.arange(NBLK, dtype=jnp.int32)[:, None, None]
    offsets = jnp.arange(1, window_span + 1, dtype=jnp.int32)[None, None, :]
    scores = jax.random.randint(order_key, (NBLK, KVH, window_span), 0, 1 << 20, dtype=jnp.int32) * window_span + offsets - 1
    scores = jnp.where(blocks - offsets >= 0, scores, -offsets)
    top_values, picked = lax.top_k(scores, SEL)
    chosen_ids = blocks - 1 - picked.astype(jnp.int32)
    live_count = jax.random.randint(count_key, (NBLK, KVH, 1), SEL // 2, SEL + 1, dtype=jnp.int32)
    slot_index = jnp.arange(SEL, dtype=jnp.int32)[None, None, :]
    keep_mask = (slot_index < live_count) & (chosen_ids >= 0)
    return jnp.where(keep_mask, chosen_ids, blocks)


def steps_of(stream_key, shape, shards, least, largest):
    factor_of = 1.0
    for dim, parts in shards:
        steps = jax.random.uniform(jax.random.fold_in(jax.random.fold_in(stream_key, 6), dim), (parts,), jnp.float32, least / len(shards), largest / len(shards))
        factor_of = factor_of * jnp.repeat(jnp.exp(steps), shape[dim] // parts).reshape((-1,) + (1,) * (len(shape) - 1 - dim))
    return factor_of


def gaussian(stream_key, shape, width, reach, split=(), kind=jnp.bfloat16):
    level = steps_of(stream_key, shape, split, -0.22, 0.18) if split else 1.0
    entries = jax.random.normal(stream_key, shape, jnp.float32) * width * level
    return jnp.minimum(jnp.maximum(entries, -reach), reach).astype(kind)


def setup_inputs(seed: int = 0) -> dict:
    splits = jax.random.split(jax.random.key(seed), 8)
    queries = gaussian(splits[0], (TOKENS, HEADS * HDIM), 1.0, 6.0, ((0, 16), (1, 2)))
    keys = gaussian(splits[1], (TOKENS, KVH * HDIM), 1.0, 6.0, ((0, 16), (1, 2)))
    values = gaussian(splits[2], (TOKENS, KVH * HDIM), 1.0, 6.0, ((0, 16), (1, 2)))
    log_sums = jnp.clip(6.0 + 1.5 * jax.random.uniform(splits[3], (HEADS, TOKENS), jnp.float32) ** steps_of(splits[3], (HEADS, TOKENS), ((0, 2), (1, 16)), -0.2, 0.2), 6.0, 7.5)
    out_grad = gaussian(splits[4], (TOKENS, HEADS * HDIM), 1.0, 6.0, ((0, 16), (1, 2)))
    chosen = draw_chosen(jax.random.fold_in(splits[7], 71), 0)
    inputs = gaussian(splits[6], (TOKENS, D), 1.0, 6.0, ((0, 16), (1, 2)))
    return {"queries": queries, "keys": keys, "values": values, "log_sums": log_sums, "out_grad": out_grad, "chosen": chosen, "inputs": inputs}


def rounded(tensor):
    return lax.optimization_barrier(tensor.astype(jnp.bfloat16)).astype(jnp.float32)


def reference(queries, keys, values, log_sums, out_grad, chosen, inputs):
    scaling = HDIM ** -0.5
    query_tile_set = queries.reshape(NBLK, BLK, KVH, QPK, HDIM)
    gradient_tiles = out_grad.reshape(NBLK, BLK, KVH, QPK, HDIM)
    sum_tiles = log_sums.reshape(KVH, QPK, NBLK, BLK).transpose(2, 0, 1, 3)
    key_tiles = keys.reshape(NBLK, BLK, KVH, HDIM)
    value_tiles = values.reshape(NBLK, BLK, KVH, HDIM)
    head_ids = jnp.arange(KVH, dtype=jnp.int32)[:, None]
    offsets = jnp.arange(BLK, dtype=jnp.int32)
    causal = (offsets[None, :] <= offsets[:, None])[None, :, None, :]

    def visit(carry, index):
        key_acc, value_acc = carry
        listed = chosen[index]
        live_slots = listed < index
        sel_keys = key_tiles[listed, :, head_ids]
        sel_values = value_tiles[listed, :, head_ids]
        own_keys = lax.dynamic_index_in_dim(key_tiles, index, 0, keepdims=False).transpose(1, 0, 2)[:, None]
        own_values = lax.dynamic_index_in_dim(value_tiles, index, 0, keepdims=False).transpose(1, 0, 2)[:, None]
        all_keys = jnp.concatenate([sel_keys, own_keys], 1).reshape(KVH, (SEL + 1) * BLK, HDIM).astype(jnp.float32)
        all_values = jnp.concatenate([sel_values, own_values], 1).reshape(KVH, (SEL + 1) * BLK, HDIM).astype(jnp.float32)
        mask_sel = jnp.broadcast_to(live_slots[:, None, :, None], (KVH, BLK, SEL, BLK))
        mask_own = jnp.broadcast_to(causal, (KVH, BLK, 1, BLK))
        permitted_mask = jnp.concatenate([mask_sel, mask_own], 2).reshape(KVH, BLK, (SEL + 1) * BLK)
        query_rows = lax.dynamic_index_in_dim(query_tile_set, index, 0, keepdims=False).astype(jnp.float32)
        grad_rows = lax.dynamic_index_in_dim(gradient_tiles, index, 0, keepdims=False).astype(jnp.float32)
        sum_rows = lax.dynamic_index_in_dim(sum_tiles, index, 0, keepdims=False)
        scores = jnp.einsum('qhgd,hkd->hgqk', query_rows, all_keys) * scaling
        weights = jnp.where(permitted_mask[:, None], jnp.exp(scores - sum_rows[..., None]), 0.0)
        grad_weights = jnp.einsum('qhgd,hkd->hgqk', grad_rows, all_values)
        delta_rows = jnp.sum(weights * grad_weights, -1, keepdims=True)
        score_gradient = rounded(weights * (grad_weights - delta_rows))
        weights_reduced = rounded(weights)
        query_part = jnp.einsum('hgqk,hkd->qhgd', score_gradient, all_keys) * scaling
        key_part = (jnp.einsum('hgqk,qhgd->hkd', score_gradient, query_rows) * scaling).reshape(KVH, SEL + 1, BLK, HDIM)
        value_part = jnp.einsum('hgqk,qhgd->hkd', weights_reduced, grad_rows).reshape(KVH, SEL + 1, BLK, HDIM)
        key_acc = key_acc.at[listed, :, head_ids].add(key_part[:, :SEL])
        key_acc = key_acc.at[index].add(key_part[:, SEL].transpose(1, 0, 2))
        value_acc = value_acc.at[listed, :, head_ids].add(value_part[:, :SEL])
        value_acc = value_acc.at[index].add(value_part[:, SEL].transpose(1, 0, 2))
        return (key_acc, value_acc), query_part.reshape(BLK, HEADS * HDIM).astype(jnp.bfloat16)

    zeros_acc = jnp.zeros((NBLK, BLK, KVH, HDIM), jnp.float32)
    (key_acc, value_acc), query_blocks = lax.scan(visit, (zeros_acc, zeros_acc), jnp.arange(NBLK, dtype=jnp.int32))
    query_grad = query_blocks.reshape(TOKENS, HEADS * HDIM)
    key_grad = key_acc.reshape(TOKENS, KVH * HDIM).astype(jnp.bfloat16)
    value_grad = value_acc.reshape(TOKENS, KVH * HDIM).astype(jnp.bfloat16)
    weight_grad = jnp.dot(inputs.T, value_grad, preferred_element_type=jnp.float32)
    return (query_grad, key_grad, value_grad, weight_grad)
```

```python
import functools

import jax
import jax.numpy as jnp
from jax import lax
from jax.experimental import pallas as pl
from jax.experimental.pallas import tpu as pltpu
from jax.sharding import PartitionSpec as P

REACH = 4
BACK = REACH // 2
SPAN = BACK + 1
MASKED = -1e30
NO_BLOCK = -(1 << 20)
LOG2E = 1.4426950408889634
MESH = pl.DeviceIdType.MESH
NT = (((1,), (1,)), ((), ()))
scope = jax.named_scope


def kernel(
    nk,
    nt,
    chosen_hbm,
    lse_hbm,
    k_hbm,
    v_hbm,
    q_hbm,
    do_hbm,
    x_hbm,
    qg_ref,
    kg_ref,
    vg_ref,
    wg_ref,
    chosen_s,
    lse_s,
    q6,
    do6,
    x_s,
    kw,
    vw,
    kt,
    bias_own,
    bias_out,
    bias_sib,
    own_bias,
    p_s,
    t_s,
    pb_s,
    ds_own,
    ds_sib,
    dv_acc,
    dvo,
    dvi,
    dk_acc,
    dko,
    dki,
    dl_out,
    dl_in,
    dt_out,
    dt_in,
    dq_out,
    dq_in,
    x_t,
    x_in,
    vall,
    late,
    po,
    ri,
    ld_sem,
    q_ld,
    do_ld,
    k_send,
    k_recv,
    v_send,
    v_recv,
    dv_send,
    dv_recv,
    dk_send,
    dk_recv,
    sib_send,
    sib_recv,
    x_send,
    x_recv,
    vg_send,
    vg_recv,
    late_send,
    late_recv,
    rs_send,
    rs_recv,
):
    me = lax.axis_index("kv")
    tp = lax.axis_index("tp")
    core = lax.rem(me, 2)
    chip = me // 2
    sib = me + 1 - 2 * core
    chips = nk // 2
    heads, _, hd = q6.shape[1:]
    tok = kw.shape[1]
    nblk = chosen_s.shape[0]
    blk = tok // nblk
    scale = hd**-0.5
    per_tp, _, rw, _ = x_t.shape
    half = per_tp // 2
    part_rows = half // 2
    f32, bf = jnp.float32, jnp.bfloat16

    barrier = pltpu.get_barrier_semaphore()

    @pl.loop(1, chips)
    def _(j):
        pl.semaphore_signal(
            barrier,
            inc=1,
            device_id=(lax.rem(chip + j, chips) * 2 + core, tp),
            device_id_type=MESH,
        )

    pl.semaphore_signal(barrier, inc=1, device_id=(sib, tp), device_id_type=MESH)
    for dt in range(1, nt):
        for kv in (me, sib):
            pl.semaphore_signal(
                barrier, inc=1, device_id=(kv, lax.rem(tp + dt, nt)), device_id_type=MESH
            )

    load_k, load_v, load_x, load_chosen, load_lse = (
        pltpu.make_async_copy(src, dst, ld_sem.at[i])
        for i, (src, dst) in enumerate(
            (
                (k_hbm, kw.at[0]),
                (v_hbm, vw.at[0]),
                (x_hbm, x_s),
                (chosen_hbm, chosen_s),
                (lse_hbm, lse_s.at[0]),
            )
        )
    )
    load_q = [
        pltpu.make_async_copy(q_hbm.at[:, pl.ds(a * hd, hd)], q6.at[0, a], q_ld.at[a])
        for a in range(heads)
    ]
    load_do = [
        pltpu.make_async_copy(do_hbm.at[:, pl.ds(a * hd, hd)], do6.at[0, a], do_ld.at[a])
        for a in range(heads)
    ]
    for load in (load_k, load_chosen, *load_q, load_lse, load_v, *load_do, load_x):
        load.start()

    def remote(src, dst, send, recv, kv, t=None):
        return pltpu.make_async_remote_copy(
            src_ref=src,
            dst_ref=dst,
            send_sem=send,
            recv_sem=recv,
            device_id=(kv, tp if t is None else t),
            device_id_type=MESH,
        )

    def k_copy(d):
        return remote(kw.at[0], kw.at[d], k_send.at[d], k_recv.at[d], me + 2 * d)

    def v_copy(d):
        return remote(vw.at[0], vw.at[d], v_send.at[d], v_recv.at[d], me + 2 * d)

    def dv_copy(d):
        return remote(dvo.at[d], dvi.at[d], dv_send.at[d], dv_recv.at[d], me - 2 * d)

    def dk_copy(d):
        return remote(dko.at[d], dki.at[d], dk_send.at[d], dk_recv.at[d], me - 2 * d)

    def to_sib(i, src, dst):
        return remote(src, dst, sib_send.at[i], sib_recv.at[i], sib)

    send_q = to_sib(0, q6.at[0], q6.at[1])
    send_lse = to_sib(1, lse_s.at[0], lse_s.at[1])
    send_bias = to_sib(2, bias_out, bias_sib)
    send_do = to_sib(3, do6.at[0], do6.at[1])
    send_x = to_sib(4, x_t.at[:, 1 - core], x_in.at[tp, core])
    send_dl = to_sib(5, dl_out, dl_in)
    send_dt = to_sib(6, dt_out, dt_in)
    send_dq = [
        to_sib(7 + i, dq_out.at[pl.ds(i * heads // 2, heads // 2)], dq_in.at[pl.ds(i * heads // 2, heads // 2)])
        for i in range(2)
    ]

    with scope("barrier_wait"):
        pl.semaphore_wait(barrier, chips + 2 * (nt - 1))

    load_k.wait()
    for d in range(1, SPAN):

        @pl.when(chip + d < chips)
        def _():
            k_copy(d).start()

    for load in load_q:
        load.wait()
    send_q.start()
    load_lse.wait()
    send_lse.start()
    load_v.wait()
    for d in range(1, SPAN):

        @pl.when(chip + d < chips)
        def _():
            v_copy(d).start()

    load_chosen.wait()
    with scope("bias"):
        row = lax.broadcasted_iota(jnp.int32, (nblk, tok), 0)
        pos = lax.broadcasted_iota(jnp.int32, (1, tok), 1)
        lists = []
        for slot in range(chosen_s.shape[2]):
            ids = jnp.full((1, tok), NO_BLOCK, jnp.int32)
            for b in range(nblk):
                block = chosen_s[b, 0, slot]
                block = jnp.where(block < me * nblk + b, block, NO_BLOCK)
                ids = jnp.where(pos >= b * blk, block, ids)
            lists.append(ids)
        lists.append(me * nblk + pos // blk)
        for o in range(REACH + 1):
            ids = row + (me - o) * nblk
            hit = ids == lists[0]
            for other in lists[1:]:
                hit = hit | (ids == other)
            marked = jnp.where(hit, 0.0, MASKED)
            if o % 2:
                bias_out[o // 2] = marked
            else:
                bias_own[o // 2] = marked
        key_row = lax.broadcasted_iota(jnp.int32, (blk, tok), 0)
        query = lax.broadcasted_iota(jnp.int32, (blk, tok), 1)
        for j in range(nblk):
            own_bias[j * blk : (j + 1) * blk, :] = jnp.where(
                key_row + j * blk > query, MASKED, bias_own[0, j : j + 1, :]
            )
    for load in load_do:
        load.wait()
    send_do.start()
    send_bias.start()

    load_x.wait()
    with scope("xT"):
        x_t[...] = x_s[...].T.reshape(x_t.shape)
    early = pl.ds(0, half)
    x_copies = []
    for dt in range(1, nt):
        other = lax.rem(tp + dt, nt)
        for s, kv, par in ((0, me, core), (1, sib, 1 - core)):
            x_copies.append(
                remote(
                    x_t.at[early, par],
                    x_in.at[tp, core, early],
                    x_send.at[dt, s],
                    x_recv.at[tp, core],
                    kv,
                    other,
                )
            )
    for copy in x_copies:
        copy.start()
    send_x.start()

    zero = jnp.zeros((tok, hd), bf)
    for d in range(1, SPAN):

        @pl.when(chip < d)
        def _():
            kw[d] = zero
            vw[d] = zero

        @pl.when(chip + d >= chips)
        def _():
            dvi[d] = zero
            dki[d] = zero

    def weights(whose, slot, d, bias, buf):
        keys = kw[d]
        for a in range(heads):
            s = lax.dot_general(keys, q6[whose, a], NT, preferred_element_type=f32)
            s = s * (scale * LOG2E)
            lse = lse_s[whose, a : a + 1, :] * LOG2E
            if bias is None:
                p = jnp.exp2(s + (own_bias[...] - lse))
            else:
                p = jnp.exp2(s.reshape(nblk, blk, tok) + (bias - lse)[:, None, :]).reshape(tok, tok)
            p_s[a, slot] = p
            pb_s[buf, :, a * tok : (a + 1) * tok] = p.astype(bf)
        return jnp.dot(
            pb_s[buf], do6[whose].reshape(heads * tok, hd), preferred_element_type=f32
        )

    with scope("tile0"):
        dv_acc[0] = weights(0, 0, 0, None, 0)

    with scope("k1_wait"):

        @pl.when(chip >= 1)
        def _():
            k_copy(1).wait_recv()

    with scope("own1"):
        own_part = weights(0, 1, 1, bias_own[1], 1)
    with scope("q_wait"):
        send_q.wait_recv()
        send_lse.wait_recv()
        send_bias.wait_recv()
        send_do.wait_recv()
    with scope("sib1"):
        near = 1 - core
        dvo[1] = (own_part + weights(1, SPAN + near, 1, bias_sib[near], 0)).astype(bf)

    @pl.when(chip >= 1)
    def _():
        dv_copy(1).start()

    with scope("k2_wait"):

        @pl.when(chip >= 2)
        def _():
            k_copy(2).wait_recv()

    with scope("tile2"):
        dv_acc[1] = weights(0, 2, 2, bias_own[2], 1)
        dv_acc[2] = weights(1, SPAN + core, 2 * core, bias_sib[core], 0)
        dvo[2] = (dv_acc[1] + jnp.where(core == 1, dv_acc[2], 0.0)).astype(bf)

    @pl.when(chip >= 2)
    def _():
        dv_copy(2).start()

    for d in range(SPAN):
        kt[d] = kw[d].T

    with scope("v_wait"):
        for d in range(1, SPAN):

            @pl.when(chip >= d)
            def _():
                v_copy(d).wait_recv()

    with scope("sib_gw"):
        for a in range(heads):
            gw = lax.dot_general(
                vw[pl.ds(core, 2)].reshape(2 * tok, hd), do6[1, a], NT, preferred_element_type=f32
            )
            t = p_s[a, SPAN:].reshape(2 * tok, tok) * gw
            t_s[a] = t
            dl_out[a : a + 1, :] = jnp.sum(t, 0, keepdims=True)
    send_dl.start()

    with scope("dv_wait"):
        for d in range(1, SPAN):

            @pl.when(chip + d < chips)
            def _():
                dv_copy(d).wait_recv()

    value = dv_acc[0] + jnp.where(core == 0, dv_acc[2], 0.0)
    for d in range(1, SPAN):
        value = value + dvi[d].astype(f32)
    value = value.astype(bf)
    vg_ref[...] = value
    vall[tp, core] = value
    vg_copies = [remote(vall.at[tp, core], vall.at[tp, core], vg_send.at[0, 1], vg_recv.at[tp, core], sib)]
    for dt in range(1, nt):
        other = lax.rem(tp + dt, nt)
        for s, kv in ((0, me), (1, sib)):
            vg_copies.append(
                remote(
                    vall.at[tp, core],
                    vall.at[tp, core],
                    vg_send.at[dt, s],
                    vg_recv.at[tp, core],
                    kv,
                    other,
                )
            )
    for copy in vg_copies:
        copy.start()

    def score_grad(a):
        gw = lax.dot_general(
            vw[...].reshape(SPAN * tok, hd), do6[0, a], NT, preferred_element_type=f32
        )
        p = p_s[a, :SPAN].reshape(SPAN * tok, tok)
        own = jnp.sum(p * gw, 0, keepdims=True)
        dt_out[a : a + 1, :] = own
        delta = own + dl_in[a : a + 1, :]
        ds_own[:, a * tok : (a + 1) * tok] = (p * (gw - delta)).astype(bf)

    with scope("dl_wait"):
        send_dl.wait_recv()
    split = heads // 2
    with scope("own_ds_a"):
        for a in range(split):
            score_grad(a)

    def rs_copy(to):
        return remote(po.at[to], ri.at[chip], rs_send.at[to], rs_recv.at[chip], to * 2 + core)

    def vg_wait(t, c):
        remote(vall.at[t, c], vall.at[t, c], vg_send.at[0, 0], vg_recv.at[t, c], sib).wait_recv()

    def send_rows(start, count):
        @pl.loop(0, count)
        def _(j):
            @pl.when(start + j != chip)
            def _():
                rs_copy(start + j).start()

    with scope("vg_wait"):
        vg_wait(tp, 1 - core)
        send_x.wait_recv()

    def own_rows(first, count, t):
        rows = pl.ds(first, count)
        return jnp.dot(
            x_t[rows, core].reshape(count * rw, tok), vall[t, core], preferred_element_type=f32
        ) + jnp.dot(
            x_in[tp, 1 - core, rows].reshape(count * rw, tok),
            vall[t, 1 - core],
            preferred_element_type=f32,
        )

    with scope("w_own"):
        for h in range(2):
            start = tp * per_tp + h * half
            po[pl.ds(start, half)] = own_rows(h * half, half, tp).astype(bf).reshape(half, rw, hd)
            send_rows(start, half)
    for dt in range(1, nt):
        t = lax.rem(tp + dt, nt)
        with scope("x_wait"):
            for c in range(2):
                remote(
                    x_t.at[early, 0], x_in.at[t, c, early], x_send.at[0, 0], x_recv.at[t, c], sib
                ).wait_recv()
        with scope("w_early"):
            start = t * per_tp
            po[pl.ds(start, half)] = (
                (
                    jnp.dot(
                        x_in[t, 0, early].reshape(half * rw, tok),
                        vall[tp, 0],
                        preferred_element_type=f32,
                    )
                    + jnp.dot(
                        x_in[t, 1, early].reshape(half * rw, tok),
                        vall[tp, 1],
                        preferred_element_type=f32,
                    )
                )
                .astype(bf)
                .reshape(half, rw, hd)
            )
            send_rows(start, half)

    with scope("own_ds_b"):
        for a in range(split, heads):
            score_grad(a)
    send_dt.start()

    def late_copy(dt, i):
        other = lax.rem(tp + dt, nt)
        rows = pl.ds(tp * per_tp + half + i * part_rows, part_rows)
        return remote(
            late.at[dt, pl.ds(i * part_rows, part_rows)],
            po.at[rows],
            late_send.at[dt, i],
            late_recv.at[tp, i],
            me,
            other,
        )

    for dt in range(1, nt):
        t = lax.rem(tp + dt, nt)
        with scope("vg_other_wait"):
            vg_wait(t, 0)
            vg_wait(t, 1)
        with scope("w_late"):
            late[dt] = own_rows(half, half, t).astype(bf).reshape(half, rw, hd)
            for i in range(2):
                late_copy(dt, i).start()

    def forward(i):
        for dt in range(1, nt):
            t = lax.rem(tp + dt, nt)
            start = t * per_tp + half + i * part_rows
            rows = pl.ds(start, part_rows)
            with scope("late_wait"):
                remote(
                    po.at[rows], po.at[rows], late_send.at[0, 0], late_recv.at[t, i], me, t
                ).wait_recv()
            send_rows(start, part_rows)

    def dk_part(ds, d, whose):
        return jnp.dot(
            ds[d * tok : (d + 1) * tok, :],
            q6[whose].reshape(heads * tok, hd),
            preferred_element_type=f32,
        )

    with scope("dk_own"):
        for d in range(1, SPAN):
            dk_acc[d] = dk_part(ds_own, d, 0)

    with scope("dt_wait"):
        send_dt.wait_recv()
    with scope("sib_ds"):
        for a in range(heads):
            delta = dl_out[a : a + 1, :] + dt_in[a : a + 1, :]
            ds_sib[:, a * tok : (a + 1) * tok] = (
                t_s[a] - p_s[a, SPAN:].reshape(2 * tok, tok) * delta
            ).astype(bf)
    with scope("dk_sib"):
        dk_acc[0] = jnp.zeros((tok, hd), f32)
        for s in range(2):
            d = core + s
            dk_acc[d] = dk_acc[d] + dk_part(ds_sib, s, 1)
        for d in range(1, SPAN):
            dko[d] = (dk_acc[d] * scale).astype(bf)
    for d in range(1, SPAN):

        @pl.when(chip >= d)
        def _():
            dk_copy(d).start()

    forward(0)
    with scope("dq_sib"):
        for i in range(2):
            for a in range(i * split, (i + 1) * split):
                dq = jnp.dot(
                    kt[core], ds_sib[:tok, a * tok : (a + 1) * tok], preferred_element_type=f32
                ) + jnp.dot(
                    kt[core + 1], ds_sib[tok:, a * tok : (a + 1) * tok], preferred_element_type=f32
                )
                dq_out[a] = (dq * scale).astype(bf)
            send_dq[i].start()
    forward(1)

    with scope("dk0"):
        key = (dk_acc[0] + dk_part(ds_own, 0, 0)) * scale

    with scope("dq_own"):
        for i in range(2):
            send_dq[i].wait_recv()
            for a in range(i * split, (i + 1) * split):
                dq = sum(
                    jnp.dot(
                        kt[d],
                        ds_own[d * tok : (d + 1) * tok, a * tok : (a + 1) * tok],
                        preferred_element_type=f32,
                    )
                    for d in range(SPAN)
                )
                dq = dq * scale + dq_in[a].astype(f32)
                qg_ref[:, a * hd : (a + 1) * hd] = dq.T.astype(bf)

    with scope("dk_wait"):
        for d in range(1, SPAN):

            @pl.when(chip + d < chips)
            def _():
                dk_copy(d).wait_recv()

            key = key + dki[d].astype(f32)
        kg_ref[...] = key.astype(bf)

    ri[pl.ds(chip, 1)] = po[pl.ds(chip, 1)]

    with scope("rs_wait"):

        @pl.loop(1, chips)
        def _(j):
            src = lax.rem(chip + j, chips)
            remote(
                po.at[src], ri.at[src], rs_send.at[src], rs_recv.at[src], src * 2 + core
            ).wait_recv()

    wg_ref[...] = jnp.sum(ri[...].astype(f32), 0)

    with scope("send_wait"):
        for d in range(1, SPAN):

            @pl.when(chip + d < chips)
            def _():
                k_copy(d).wait_send()
                v_copy(d).wait_send()

            @pl.when(chip >= d)
            def _():
                dv_copy(d).wait_send()
                dk_copy(d).wait_send()

        for copy in (
            send_q,
            send_lse,
            send_bias,
            send_do,
            send_x,
            send_dl,
            send_dt,
            *send_dq,
            *x_copies,
            *vg_copies,
        ):
            copy.wait_send()
        for dt in range(1, nt):
            for i in range(2):
                late_copy(dt, i).wait_send()

        @pl.loop(1, chips)
        def _(j):
            rs_copy(lax.rem(chip + j, chips)).wait_send()


def finish(*refs):
    count = len(refs) // 2
    sems = refs[-1]
    copies = [
        pltpu.make_async_copy(refs[i], refs[count + i], sems.at[i]) for i in range(count)
    ]
    for copy in copies:
        copy.start()
    for copy in copies:
        copy.wait()


def shards(nk, nt, queries, keys, values, log_sums, out_grad, chosen, inputs):
    tok, hd = keys.shape
    heads = queries.shape[1] // hd
    nblk = chosen.shape[0]
    feats = inputs.shape[1]
    rw = feats * nt // nk
    per_tp = feats // (2 * rw)
    bf, f32 = jnp.bfloat16, jnp.float32
    dma = pltpu.SemaphoreType.DMA
    vmem = pl.BlockSpec(memory_space=pltpu.VMEM)
    hbm = pl.BlockSpec(memory_space=pl.ANY)
    chips = nk // 2
    parts = pl.pallas_call(
        functools.partial(kernel, nk, nt),
        out_shape=(
            jax.ShapeDtypeStruct((tok, heads * hd), bf),
            jax.ShapeDtypeStruct((tok, hd), bf),
            jax.ShapeDtypeStruct((tok, hd), bf),
            jax.ShapeDtypeStruct((rw, hd), f32),
        ),
        in_specs=[hbm] * 7,
        out_specs=(vmem, vmem, vmem, vmem),
        scratch_shapes=[
            pltpu.SMEM(chosen.shape, jnp.int32),
            pltpu.VMEM((2, heads, tok), f32),
            pltpu.VMEM((2, heads, tok, hd), bf),
            pltpu.VMEM((2, heads, tok, hd), bf),
            pltpu.VMEM((tok, feats), bf),
            pltpu.VMEM((SPAN, tok, hd), bf),
            pltpu.VMEM((SPAN, tok, hd), bf),
            pltpu.VMEM((SPAN, hd, tok), bf),
            pltpu.VMEM((SPAN, nblk, tok), f32),
            pltpu.VMEM((2, nblk, tok), f32),
            pltpu.VMEM((2, nblk, tok), f32),
            pltpu.VMEM((tok, tok), f32),
            pltpu.VMEM((heads, SPAN + 2, tok, tok), f32),
            pltpu.VMEM((heads, 2 * tok, tok), f32),
            pltpu.VMEM((2, tok, heads * tok), bf),
            pltpu.VMEM((SPAN * tok, heads * tok), bf),
            pltpu.VMEM((2 * tok, heads * tok), bf),
            pltpu.VMEM((SPAN, tok, hd), f32),
            pltpu.VMEM((SPAN, tok, hd), bf),
            pltpu.VMEM((SPAN, tok, hd), bf),
            pltpu.VMEM((SPAN, tok, hd), f32),
            pltpu.VMEM((SPAN, tok, hd), bf),
            pltpu.VMEM((SPAN, tok, hd), bf),
            pltpu.VMEM((heads, tok), f32),
            pltpu.VMEM((heads, tok), f32),
            pltpu.VMEM((heads, tok), f32),
            pltpu.VMEM((heads, tok), f32),
            pltpu.VMEM((heads, hd, tok), bf),
            pltpu.VMEM((heads, hd, tok), bf),
            pltpu.VMEM((per_tp, 2, rw, tok), bf),
            pltpu.VMEM((nt, 2, per_tp, rw, tok), bf),
            pltpu.VMEM((nt, 2, tok, hd), bf),
            pltpu.VMEM((nt, per_tp // 2, rw, hd), bf),
            pltpu.VMEM((chips, rw, hd), bf),
            pltpu.VMEM((chips, rw, hd), bf),
            dma((5,)),
            dma((heads,)),
            dma((heads,)),
            dma((SPAN,)),
            dma((SPAN,)),
            dma((SPAN,)),
            dma((SPAN,)),
            dma((SPAN,)),
            dma((SPAN,)),
            dma((SPAN,)),
            dma((SPAN,)),
            dma((9,)),
            dma((9,)),
            dma((nt, 2)),
            dma((nt, 2)),
            dma((nt, 2)),
            dma((nt, 2)),
            dma((nt, 2)),
            dma((nt, 2)),
            dma((chips,)),
            dma((chips,)),
        ],
        compiler_params=pltpu.CompilerParams(
            collective_id=0, has_side_effects=True, vmem_limit_bytes=60 * 1024 * 1024
        ),
    )(chosen, log_sums, keys, values, queries, out_grad, inputs)
    return pl.pallas_call(
        finish,
        out_shape=tuple(jax.ShapeDtypeStruct(part.shape, part.dtype) for part in parts),
        in_specs=[vmem] * len(parts),
        out_specs=(hbm,) * len(parts),
        scratch_shapes=[dma((len(parts),))],
    )(*parts)


def solution(mesh):
    in_specs = (
        P("kv", "tp"),
        P("kv", "tp"),
        P("kv", "tp"),
        P("tp", "kv"),
        P("kv", "tp"),
        P("kv", "tp", None),
        P("kv", "tp"),
    )
    out_specs = (P("kv", "tp"), P("kv", "tp"), P("kv", "tp"), P("kv", "tp"))
    return jax.shard_map(
        functools.partial(shards, mesh.shape["kv"], mesh.shape["tp"]),
        mesh=mesh,
        in_specs=in_specs,
        out_specs=out_specs,
        check_vma=False,
    )
```

```python
import functools

import jax
import jax.numpy as jnp
from jax import lax
from jax.experimental import pallas as pl
from jax.experimental.pallas import tpu as pltpu
from jax.sharding import PartitionSpec as P

REACH = 4
BACK = REACH // 2
SPAN = BACK + 1
STEPS = tuple(step for d in range(1, BACK + 1) for step in (d, -d))
LAST = 3
MASKED = -1e30
NO_BLOCK = -(1 << 20)
LOG2E = 1.4426950408889634
MESH = pl.DeviceIdType.MESH
NT = (((1,), (1,)), ((), ()))
scope = jax.named_scope


def kernel(
    nk,
    nt,
    chosen_hbm,
    lse_hbm,
    k_hbm,
    v_hbm,
    q_hbm,
    do_hbm,
    x_hbm,
    qg_ref,
    kg_ref,
    vg_ref,
    wg_ref,
    chosen_s,
    lse_s,
    q6,
    do6,
    x_s,
    kvw,
    kt,
    bias_own,
    bias_out,
    bias_sib,
    own_bias,
    p_s,
    t_s,
    pb_s,
    ds_own,
    ds_sib,
    dv_own,
    dv_far,
    dk_acc,
    back_out,
    back_in,
    dl_out,
    dl_in,
    dt_out,
    dt_in,
    dq_out,
    dq_in,
    x_t,
    x_in,
    vall,
    late,
    late_in,
    pf,
    po,
    yi,
    zo,
    ri,
    ld_sem,
    kv_send,
    k_recv,
    v_recv,
    back_send,
    dv_recv,
    dk_recv,
    sib_send,
    sib_recv,
    x_send,
    x_recv,
    vg_send,
    vg_recv,
    late_send,
    late_recv,
    y_send,
    y_recv,
    rs_send,
    rs_recv,
    go_sem,
):
    me = lax.axis_index("kv")
    tp = lax.axis_index("tp")
    core = lax.rem(me, 2)
    chip = me // 2
    sib = me + 1 - 2 * core
    side = lax.rem(chip, 2)
    across = me + 2 - 4 * side
    chips = nk // 2
    _, heads, tok, hd = q6.shape
    kw, vw = kvw.at[0], kvw.at[1]
    dvo, dko = back_out.at[0], back_out.at[1]
    dvi, dki = back_in.at[0], back_in.at[1]
    nblk = chosen_s.shape[0]
    blk = tok // nblk
    scale = hd**-0.5
    per_tp, _, rw, _ = x_t.shape
    half = per_tp // 2
    pairs = chips // 2
    hh = half // 2
    mine = chip // 2
    half_heads = heads // 2
    mid = 1 - lax.rem(tp, 2)
    f32, bf = jnp.float32, jnp.bfloat16

    behind = chip
    ahead = chips - 1 - chip
    near_chips = [(step, ahead >= step if step > 0 else behind >= -step) for step in STEPS]
    barrier = pltpu.get_barrier_semaphore()
    count = 1 + 3 * (nt - 1)
    for step, exists in near_chips:
        count = count + jnp.where(exists, 1, 0)

        @pl.when(exists)
        def _():
            pl.semaphore_signal(
                barrier, inc=1, device_id=(me + 2 * step, tp), device_id_type=MESH
            )

    pl.semaphore_signal(barrier, inc=1, device_id=(sib, tp), device_id_type=MESH)
    for dt in range(1, nt):
        for kv in (me, sib, across):
            pl.semaphore_signal(
                barrier, inc=1, device_id=(kv, lax.rem(tp + dt, nt)), device_id_type=MESH
            )

    load_k, load_v, load_x, load_chosen, load_lse = (
        pltpu.make_async_copy(src, dst, ld_sem.at[i])
        for i, (src, dst) in enumerate(
            (
                (k_hbm, kw.at[0]),
                (v_hbm, vw.at[0]),
                (x_hbm, x_s),
                (chosen_hbm, chosen_s),
                (lse_hbm, lse_s.at[0]),
            )
        )
    )
    load_q, load_do = (
        [
            pltpu.make_async_copy(src.at[:, pl.ds(a * hd, hd)], dst.at[0, a], ld_sem.at[i])
            for a in range(heads)
        ]
        for i, src, dst in ((5, q_hbm, q6), (6, do_hbm, do6))
    )

    def all_of(ref, sem):
        return pltpu.make_async_copy(ref, ref, sem)

    for load in (load_k, load_chosen, *load_q, load_lse, load_v, *load_do, load_x):
        load.start()

    def remote(src, dst, send, recv, kv, t=None):
        return pltpu.make_async_remote_copy(
            src_ref=src,
            dst_ref=dst,
            send_sem=send,
            recv_sem=recv,
            device_id=(kv, tp if t is None else t),
            device_id_type=MESH,
        )

    def k_copy(d):
        return remote(kw.at[0], kw.at[d], kv_send, k_recv.at[d - 1], me + 2 * d)

    def v_copy(d):
        return remote(vw.at[0], vw.at[d], kv_send, v_recv, me + 2 * d)

    def dv_copy(d):
        return remote(dvo.at[d - 1], dvi.at[d - 1], back_send, dv_recv, me - 2 * d)

    def dk_copy(d):
        return remote(dko.at[d - 1], dki.at[d - 1], back_send, dk_recv, me - 2 * d)

    def each_count(left, wait):
        for count in range(1, BACK + 1):
            here = (left == count) if count < BACK else (left >= count)

            @pl.when(here)
            def _():
                wait(pl.ds(0, count))

    def to_sib(i, j, src, dst):
        return remote(src, dst, sib_send.at[i], sib_recv.at[j], sib)

    send_q = to_sib(0, 0, q6.at[0], q6.at[1])
    send_do = to_sib(0, 0, do6.at[0], do6.at[1])
    send_lse = to_sib(1, 1, lse_s.at[0], lse_s.at[1])
    send_bias = to_sib(2, 2, bias_out, bias_sib)
    send_x = to_sib(3, 3, x_t.at[:, 1 - core], x_in.at[tp, core])
    send_dl = to_sib(4, 4, dl_out, dl_in)
    send_dt = to_sib(4, 5, dt_out, dt_in)
    send_dq = [
        to_sib(5, 6 + i, dq_out.at[pl.ds(i * half_heads, half_heads)], dq_in.at[pl.ds(i * half_heads, half_heads)])
        for i in range(2)
    ]

    with scope("barrier_wait"):
        pl.semaphore_wait(barrier, count)

    def relay(point):
        for i, step, left, done in ((0, -BACK, ahead, behind), (1, BACK, behind, ahead)):
            hops = left // BACK
            turn = hops == point if point < LAST else hops >= point

            @pl.when(turn & (hops > 0))
            def _():
                pl.semaphore_wait(go_sem.at[i], 1)

            @pl.when(turn & (done >= BACK))
            def _():
                pl.semaphore_signal(
                    go_sem.at[i], inc=1, device_id=(me + 2 * step, tp), device_id_type=MESH
                )

    load_k.wait()
    for d in range(1, SPAN):

        @pl.when(chip + d < chips)
        def _():
            k_copy(d).start()

    relay(0)
    all_of(q6.at[0], ld_sem.at[5]).wait()
    send_q.start()
    load_lse.wait()
    send_lse.start()
    load_v.wait()
    for d in range(1, SPAN):

        @pl.when(chip + d < chips)
        def _():
            v_copy(d).start()

    load_chosen.wait()
    with scope("bias"):
        row = lax.broadcasted_iota(jnp.int32, (nblk, tok), 0)
        pos = lax.broadcasted_iota(jnp.int32, (1, tok), 1)
        lists = []
        for slot in range(chosen_s.shape[2]):
            ids = jnp.full((1, tok), NO_BLOCK, jnp.int32)
            for b in range(nblk):
                block = chosen_s[b, 0, slot]
                block = jnp.where(block < me * nblk + b, block, NO_BLOCK)
                ids = jnp.where(pos >= b * blk, block, ids)
            lists.append(ids)
        lists.append(me * nblk + pos // blk)
        for o in range(REACH + 1):
            ids = row + (me - o) * nblk
            hit = ids == lists[0]
            for other in lists[1:]:
                hit = hit | (ids == other)
            marked = jnp.where(hit, 0.0, MASKED)
            if o % 2:
                bias_out[o // 2] = marked
            else:
                bias_own[o // 2] = marked
        key_row = lax.broadcasted_iota(jnp.int32, (blk, tok), 0)
        query = lax.broadcasted_iota(jnp.int32, (blk, tok), 1)
        for j in range(nblk):
            own_bias[j * blk : (j + 1) * blk, :] = jnp.where(
                key_row + j * blk > query, MASKED, bias_own[0, j : j + 1, :]
            )
    all_of(do6.at[0], ld_sem.at[6]).wait()
    send_do.start()
    send_bias.start()

    load_x.wait()
    with scope("xT"):
        x_t[...] = x_s[...].T.reshape(x_t.shape)

    def end_rows(t):
        return pl.ds(lax.rem(t, 2) * half, half)

    early = end_rows(tp)
    x_copies = []
    for dt in range(1, nt):
        other = lax.rem(tp + dt, nt)
        for s, kv, par in ((0, me, core), (1, sib, 1 - core)):
            x_copies.append(
                remote(
                    x_t.at[early, par],
                    x_in.at[tp, core, early],
                    x_send.at[dt - 1],
                    x_recv.at[nt - dt - 1],
                    kv,
                    other,
                )
            )
    for copy in x_copies:
        copy.start()

    zero = jnp.zeros((tok, hd), bf)
    for d in range(1, SPAN):

        @pl.when(chip < d)
        def _():
            kw[d] = zero
            vw[d] = zero

        @pl.when(chip + d >= chips)
        def _():
            dvi[d - 1] = zero
            dki[d - 1] = zero

    def weights(whose, slot, d, bias, buf):
        keys = kw[d]
        for a in range(heads):
            s = lax.dot_general(keys, q6[whose, a], NT, preferred_element_type=f32)
            s = s * (scale * LOG2E)
            lse = lse_s[whose, a : a + 1, :] * LOG2E
            if bias is None:
                p = jnp.exp2(s + (own_bias[...] - lse))
            else:
                p = jnp.exp2(s.reshape(nblk, blk, tok) + (bias - lse)[:, None, :]).reshape(tok, tok)
            p_s[a, slot] = p
            pb_s[buf, :, a * tok : (a + 1) * tok] = p.astype(bf)
        return jnp.dot(
            pb_s[buf], do6[whose].reshape(heads * tok, hd), preferred_element_type=f32
        )

    near = 1 - core
    far = 2 * core

    def far_tile():
        dv_far[...] = weights(1, SPAN + 1, far, bias_sib[core], 0)

    with scope("tile0"):
        dv_own[...] = weights(0, 0, 0, None, 0)

    with scope("q_wait"):
        all_of(q6, sib_recv.at[0]).wait()
        send_lse.wait_recv()
        send_bias.wait_recv()

    relay(1)

    @pl.when(core == 0)
    def _():
        with scope("far0"):
            far_tile()

    def tile1():
        with scope("k1_wait"):

            @pl.when(chip >= 1)
            def _():
                k_copy(1).wait_recv()

        with scope("d1"):
            dvo[0] = (
                weights(0, 1, 1, bias_own[1], 1) + weights(1, SPAN, 1, bias_sib[near], 0)
            ).astype(bf)

        @pl.when(chip >= 1)
        def _():
            dv_copy(1).start()

    def tile2():
        with scope("k2_wait"):

            @pl.when(chip >= 2)
            def _():
                k_copy(2).wait_recv()

        @pl.when(core == 1)
        def _():
            with scope("far1"):
                far_tile()

        with scope("d2"):
            dvo[1] = (
                weights(0, 2, 2, bias_own[2], 1) + jnp.where(core == 1, dv_far[...], 0.0)
            ).astype(bf)

        @pl.when(chip >= 2)
        def _():
            dv_copy(2).start()

    @pl.when(side == 0)
    def _():
        tile2()
        tile1()

    @pl.when(side == 1)
    def _():
        tile1()
        tile2()

    send_x.start()
    relay(2)
    for d in range(SPAN):
        kt[d] = kw[d].T

    with scope("v_wait"):
        each_count(behind, lambda rows: all_of(vw.at[rows], v_recv).wait())

    with scope("sib_gw"):
        for a in range(heads):
            total = jnp.zeros((1, tok), f32)
            for i, d in enumerate((1, far)):
                gw = lax.dot_general(vw[d], do6[1, a], NT, preferred_element_type=f32)
                t = p_s[a, SPAN + i] * gw
                t_s[a, i] = t
                total = total + jnp.sum(t, 0, keepdims=True)
            dl_out[a : a + 1, :] = total
    send_dl.start()

    with scope("dv_wait"):
        each_count(ahead, lambda rows: all_of(dvi.at[rows], dv_recv).wait())

    value = dv_own[...] + jnp.where(core == 0, dv_far[...], 0.0)
    for d in range(1, SPAN):
        value = value + dvi[d - 1].astype(f32)
    value = value.astype(bf)
    vg_ref[...] = value
    vall[tp * 2 + core] = value
    my_vg = vall.at[tp * 2 + core]
    vg_copies = [remote(my_vg, my_vg, vg_send, vg_recv.at[tp * 2 + core], sib)]
    for dt in range(1, nt):
        for kv in (me, sib):
            vg_copies.append(
                remote(my_vg, my_vg, vg_send, vg_recv.at[tp * 2 + core], kv, lax.rem(tp + dt, nt))
            )
    for copy in vg_copies:
        copy.start()

    def score_grad(a):
        gw = lax.dot_general(
            vw[...].reshape(SPAN * tok, hd), do6[0, a], NT, preferred_element_type=f32
        )
        p = p_s[a, :SPAN].reshape(SPAN * tok, tok)
        own = jnp.sum(p * gw, 0, keepdims=True)
        dt_out[a : a + 1, :] = own
        delta = own + dl_in[a : a + 1, :]
        ds_own[:, a * tok : (a + 1) * tok] = (p * (gw - delta)).astype(bf)

    with scope("dl_wait"):
        send_dl.wait_recv()
    split = heads // 2
    with scope("own_ds_a"):
        for a in range(split):
            score_grad(a)

    def rs_copy(m):
        return remote(zo.at[m], ri.at[mine], rs_send, rs_recv, (2 * m + side) * 2 + core)

    def vg_wait(t, c):
        all_of(vall.at[t * 2 + c], vg_recv.at[t * 2 + c]).wait()

    def y_copy(g, first):
        rows = pl.ds(first // 2, hh)
        return remote(po.at[rows, 1 - side], yi.at[rows], y_send, y_recv.at[g], across)

    def put_rows(g, first, part):
        rows = pl.ds(first // 2, hh)
        pf[rows] = part.reshape(hh, 2, rw, hd)
        po[rows] = part.astype(bf).reshape(hh, 2, rw, hd)
        y_copy(g, first).start()

    def pass_rows(first):
        @pl.loop(0, hh)
        def _(j):
            @pl.when(first // 2 + j != mine)
            def _():
                rs_copy(first // 2 + j).start()

    def join_rows(g, first):
        with scope(f"y_wait{g}"):
            y_copy(g, first).wait_recv()
        rows = pl.ds(first // 2, hh)
        zo[rows] = (pf[rows, side] + yi[rows].astype(f32)).astype(bf)
        pass_rows(first)

    with scope("vg_wait"):
        vg_wait(tp, 1 - core)
        send_x.wait_recv()

    def own_rows(first, t):
        rows = pl.ds(first, half)
        return jnp.dot(
            x_t[rows, core].reshape(half * rw, tok), vall[t * 2 + core], preferred_element_type=f32
        ) + jnp.dot(
            x_in[tp, 1 - core, rows].reshape(half * rw, tok),
            vall[t * 2 + 1 - core],
            preferred_element_type=f32,
        )

    with scope("relay"):
        relay(LAST)
    groups = []
    with scope("w_end"):
        first = tp * per_tp + (1 - mid) * half
        put_rows(0, first, own_rows((1 - mid) * half, tp))
        groups.append((0, first))
    with scope("w_mid"):
        first = tp * per_tp + mid * half
        put_rows(nt, first, own_rows(mid * half, tp))
        groups.append((nt, first))

    with scope("own_ds_b"):
        for a in range(split, heads):
            score_grad(a)
    send_dt.start()

    def dk_part(ds, d, whose):
        return jnp.dot(
            ds[d * tok : (d + 1) * tok, :],
            q6[whose].reshape(heads * tok, hd),
            preferred_element_type=f32,
        )

    with scope("dk_own"):
        for d in range(1, SPAN):
            dk_acc[d - 1] = dk_part(ds_own, d, 0)

    for dt in range(1, nt):
        t = lax.rem(tp + dt, nt)
        rows = end_rows(t)
        with scope("x_wait"):
            all_of(x_in.at[t, :, rows], x_recv.at[dt - 1]).wait()
        with scope("w_early"):
            part = sum(
                jnp.dot(
                    x_in[t, c, rows].reshape(half * rw, tok),
                    vall[tp * 2 + c],
                    preferred_element_type=f32,
                )
                for c in range(2)
            )
            first = t * per_tp + lax.rem(t, 2) * half
            put_rows(dt, first, part)
            groups.append((dt, first))

    with scope("dt_wait"):
        send_dt.wait_recv()
    with scope("sib_ds"):
        for a in range(heads):
            delta = dl_out[a : a + 1, :] + dt_in[a : a + 1, :]
            for i in range(2):
                ds_sib[i * tok : (i + 1) * tok, a * tok : (a + 1) * tok] = (
                    t_s[a, i] - p_s[a, SPAN + i] * delta
                ).astype(bf)
    with scope("dk_sib"):
        dko[0] = ((dk_acc[0] + dk_part(ds_sib, 0, 1)) * scale).astype(bf)
        dk_far = dk_part(ds_sib, 1, 1)
        dko[1] = ((dk_acc[1] + jnp.where(core == 1, dk_far, 0.0)) * scale).astype(bf)
        dk_acc[0] = jnp.where(core == 0, dk_far, 0.0)
    for d in range(1, SPAN):

        @pl.when(chip >= d)
        def _():
            dk_copy(d).start()

    def late_copy(dt, i):
        return remote(
            late.at[dt - 1, :, side if i == 0 else 1 - side],
            late_in.at[tp, side],
            late_send,
            late_recv.at[nt - dt - 1],
            me if i == 0 else across,
            lax.rem(tp + dt, nt),
        )

    for dt in range(1, nt):
        t = lax.rem(tp + dt, nt)
        with scope("vg_other_wait"):
            vg_wait(t, 0)
            vg_wait(t, 1)
        with scope("w_late"):
            late[dt - 1] = own_rows(mid * half, t).astype(bf).reshape(hh, 2, rw, hd)
            for i in (1, 0):
                late_copy(dt, i).start()

    def join_late():
        for dt in range(1, nt):
            t = lax.rem(tp + dt, nt)
            first = t * per_tp + (1 - lax.rem(t, 2)) * half
            with scope("late_wait"):
                all_of(late_in.at[t], late_recv.at[dt - 1]).wait()
            zo[pl.ds(first // 2, hh)] = (
                late_in[t, 0].astype(f32) + late_in[t, 1].astype(f32)
            ).astype(bf)
            pass_rows(first)

    def query_sib(i):
        with scope("dq_sib"):
            for a in range(i * split, (i + 1) * split):
                cols = pl.ds(a * tok, tok)
                dq = jnp.dot(kt[1], ds_sib[:tok, cols], preferred_element_type=f32) + jnp.dot(
                    kt[far], ds_sib[tok:, cols], preferred_element_type=f32
                )
                dq_out[a] = (dq * scale).astype(bf)
        send_dq[i].start()

    for group in groups[:2]:
        join_rows(*group)
    query_sib(0)
    query_sib(1)
    for group in groups[2:]:
        join_rows(*group)
    with scope("dk0"):
        key = (dk_acc[0] + dk_part(ds_own, 0, 0)) * scale
    join_late()

    with scope("dq_own"):
        for i in range(2):
            send_dq[i].wait_recv()
            for a in range(i * split, (i + 1) * split):
                dq = sum(
                    jnp.dot(
                        kt[d],
                        ds_own[d * tok : (d + 1) * tok, a * tok : (a + 1) * tok],
                        preferred_element_type=f32,
                    )
                    for d in range(SPAN)
                )
                dq = dq * scale + dq_in[a].astype(f32)
                qg_ref[:, a * hd : (a + 1) * hd] = dq.T.astype(bf)

    with scope("dk_wait"):
        each_count(ahead, lambda rows: all_of(dki.at[rows], dk_recv).wait())
    for d in range(BACK):
        key = key + dki[d].astype(f32)
    kg_ref[...] = key.astype(bf)

    with scope("rs_wait"):

        ri[pl.ds(mine, 1)] = zo[pl.ds(mine, 1)]
        all_of(ri.at[pl.ds(0, pairs - 1)], rs_recv).wait()
    wg_ref[...] = jnp.sum(ri[...].astype(f32), 0)

    with scope("send_wait"):
        each_count(ahead, lambda rows: all_of(kvw.at[:, rows], kv_send).wait())
        each_count(behind, lambda rows: all_of(back_out.at[:, rows], back_send).wait())
        all_of(q6, sib_send.at[0]).wait()
        send_lse.wait_send()
        send_bias.wait_send()
        send_x.wait_send()
        all_of(lse_s, sib_send.at[4]).wait()
        all_of(dq_out, sib_send.at[5]).wait()
        for dt in range(1, nt):
            all_of(x_t.at[early], x_send.at[dt - 1]).wait()
        all_of(vall.at[pl.ds(0, 2 * nt - 1)], vg_send).wait()
        all_of(late, late_send).wait()
        all_of(po.at[pl.ds(0, (nt + 1) * hh), 0], y_send).wait()
        all_of(ri.at[pl.ds(0, pairs - 1)], rs_send).wait()


def finish(*refs):
    count = len(refs) // 2
    sems = refs[-1]
    copies = [
        pltpu.make_async_copy(refs[i], refs[count + i], sems.at[i]) for i in range(count)
    ]
    for copy in copies:
        copy.start()
    for copy in copies:
        copy.wait()


def shards(nk, nt, queries, keys, values, log_sums, out_grad, chosen, inputs):
    tok, hd = keys.shape
    heads = queries.shape[1] // hd
    nblk = chosen.shape[0]
    feats = inputs.shape[1]
    rw = feats * nt // nk
    per_tp = feats // (2 * rw)
    bf, f32 = jnp.bfloat16, jnp.float32
    dma = pltpu.SemaphoreType.DMA
    vmem = pl.BlockSpec(memory_space=pltpu.VMEM)
    hbm = pl.BlockSpec(memory_space=pltpu.HBM)
    pairs = nk // 4
    parts = pl.pallas_call(
        functools.partial(kernel, nk, nt),
        out_shape=(
            pltpu.VMEM((tok, heads * hd), bf),
            pltpu.VMEM((tok, hd), bf),
            pltpu.VMEM((tok, hd), bf),
            pltpu.VMEM((rw, hd), f32),
        ),
        in_specs=[hbm] * 7,
        out_specs=(vmem, vmem, vmem, vmem),
        scratch_shapes=[
            pltpu.SMEM(chosen.shape, jnp.int32),
            pltpu.VMEM((2, heads, tok), f32),
            pltpu.VMEM((2, heads, tok, hd), bf),
            pltpu.VMEM((2, heads, tok, hd), bf),
            pltpu.VMEM((tok, feats), bf),
            pltpu.VMEM((2, SPAN, tok, hd), bf),
            pltpu.VMEM((SPAN, hd, tok), bf),
            pltpu.VMEM((SPAN, nblk, tok), f32),
            pltpu.VMEM((2, nblk, tok), f32),
            pltpu.VMEM((2, nblk, tok), f32),
            pltpu.VMEM((tok, tok), f32),
            pltpu.VMEM((heads, SPAN + 2, tok, tok), f32),
            pltpu.VMEM((heads, 2, tok, tok), f32),
            pltpu.VMEM((2, tok, heads * tok), bf),
            pltpu.VMEM((SPAN * tok, heads * tok), bf),
            pltpu.VMEM((2 * tok, heads * tok), bf),
            pltpu.VMEM((tok, hd), f32),
            pltpu.VMEM((tok, hd), f32),
            pltpu.VMEM((BACK, tok, hd), f32),
            pltpu.VMEM((2, BACK, tok, hd), bf),
            pltpu.VMEM((2, BACK, tok, hd), bf),
            pltpu.VMEM((heads, tok), f32),
            pltpu.VMEM((heads, tok), f32),
            pltpu.VMEM((heads, tok), f32),
            pltpu.VMEM((heads, tok), f32),
            pltpu.VMEM((heads, hd, tok), bf),
            pltpu.VMEM((heads, hd, tok), bf),
            pltpu.VMEM((per_tp, 2, rw, tok), bf),
            pltpu.VMEM((nt, 2, per_tp, rw, tok), bf),
            pltpu.VMEM((2 * nt, tok, hd), bf),
            pltpu.VMEM((nt - 1, per_tp // 4, 2, rw, hd), bf),
            pltpu.VMEM((nt, 2, per_tp // 4, rw, hd), bf),
            pltpu.VMEM((pairs, 2, rw, hd), f32),
            pltpu.VMEM((pairs, 2, rw, hd), bf),
            pltpu.VMEM((pairs, rw, hd), bf),
            pltpu.VMEM((pairs, rw, hd), bf),
            pltpu.VMEM((pairs, rw, hd), bf),
            dma((7,)),
            dma,
            dma((BACK,)),
            dma,
            dma,
            dma,
            dma,
            dma((6,)),
            dma((8,)),
            dma((nt - 1,)),
            dma((nt - 1,)),
            dma,
            dma((2 * nt,)),
            dma,
            dma((nt - 1,)),
            dma,
            dma((nt + 1,)),
            dma,
            dma,
            pltpu.SemaphoreType.REGULAR((2,)),
        ],
        compiler_params=pltpu.CompilerParams(
            collective_id=0, has_side_effects=True, vmem_limit_bytes=60 * 1024 * 1024
        ),
    )(chosen, log_sums, keys, values, queries, out_grad, inputs)
    return pl.pallas_call(
        finish,
        out_shape=tuple(jax.ShapeDtypeStruct(part.shape, part.dtype) for part in parts),
        in_specs=[vmem] * len(parts),
        out_specs=(hbm,) * len(parts),
        scratch_shapes=[dma((len(parts),))],
    )(*(pltpu.with_memory_space_constraint(part, pltpu.VMEM) for part in parts))


def solution(mesh):
    in_specs = (
        P("kv", "tp"),
        P("kv", "tp"),
        P("kv", "tp"),
        P("tp", "kv"),
        P("kv", "tp"),
        P("kv", "tp", None),
        P("kv", "tp"),
    )
    out_specs = (P("kv", "tp"), P("kv", "tp"), P("kv", "tp"), P("kv", "tp"))
    return jax.shard_map(
        functools.partial(shards, mesh.shape["kv"], mesh.shape["tp"]),
        mesh=mesh,
        in_specs=in_specs,
        out_specs=out_specs,
        check_vma=False,
    )
```

```python
import functools

import jax
import jax.numpy as jnp
from jax import lax
from jax.experimental import pallas as pl
from jax.experimental.pallas import tpu as pltpu
from jax.sharding import PartitionSpec as P

REACH = 4
BACK = REACH // 2
SPAN = BACK + 1
STEPS = tuple(step for d in range(1, BACK + 1) for step in (d, -d))
LAST = 3
MASKED = -1e30
NO_BLOCK = -(1 << 20)
LOG2E = 1.4426950408889634
MESH = pl.DeviceIdType.MESH
NT = (((1,), (1,)), ((), ()))
scope = jax.named_scope


def kernel(
    nk,
    nt,
    chosen_hbm,
    lse_hbm,
    k_hbm,
    v_hbm,
    q_hbm,
    do_hbm,
    x_hbm,
    qg_ref,
    kg_ref,
    vg_ref,
    wg_ref,
    chosen_s,
    lse_s,
    q6,
    do6,
    x_s,
    kvw,
    kt,
    bias_own,
    bias_out,
    bias_sib,
    own_bias,
    p_s,
    t_s,
    pb_s,
    ds_own,
    ds_sib,
    dv_own,
    dv_far,
    dk_acc,
    back_out,
    back_in,
    dk_pass,
    dk_far2,
    dl_out,
    dl_in,
    dt_out,
    dt_in,
    dq_out,
    dq_in,
    x_t,
    x_in,
    vall,
    late,
    late_in,
    pf,
    po,
    yi,
    zo,
    ri,
    ld_sem,
    kv_send,
    k_recv,
    v_recv,
    back_send,
    dv_recv,
    dk_recv,
    pass_recv,
    sib_send,
    sib_recv,
    x_send,
    x_recv,
    vg_send,
    vg_recv,
    late_send,
    late_recv,
    y_send,
    y_recv,
    rs_send,
    rs_recv,
    go_sem,
):
    me = lax.axis_index("kv")
    tp = lax.axis_index("tp")
    core = lax.rem(me, 2)
    chip = me // 2
    sib = me + 1 - 2 * core
    side = lax.rem(chip, 2)
    across = me + 2 - 4 * side
    chips = nk // 2
    _, heads, tok, hd = q6.shape
    kw, vw = kvw.at[0], kvw.at[1]
    dvo, dko = back_out.at[0], back_out.at[1]
    dvi, dki = back_in.at[0], back_in.at[1]
    nblk = chosen_s.shape[0]
    blk = tok // nblk
    scale = hd**-0.5
    per_tp, _, rw, _ = x_t.shape
    half = per_tp // 2
    pairs = chips // 2
    hh = half // 2
    mine = chip // 2
    half_heads = heads // 2
    mid = 1 - lax.rem(tp, 2)
    f32, bf = jnp.float32, jnp.bfloat16

    behind = chip
    ahead = chips - 1 - chip
    near_chips = [(step, ahead >= step if step > 0 else behind >= -step) for step in STEPS]
    barrier = pltpu.get_barrier_semaphore()
    count = 1 + 3 * (nt - 1)
    for step, exists in near_chips:
        count = count + jnp.where(exists, 1, 0)

        @pl.when(exists)
        def _():
            pl.semaphore_signal(
                barrier, inc=1, device_id=(me + 2 * step, tp), device_id_type=MESH
            )

    pl.semaphore_signal(barrier, inc=1, device_id=(sib, tp), device_id_type=MESH)
    for dt in range(1, nt):
        for kv in (me, sib, across):
            pl.semaphore_signal(
                barrier, inc=1, device_id=(kv, lax.rem(tp + dt, nt)), device_id_type=MESH
            )

    load_k, load_v, load_x, load_chosen, load_lse = (
        pltpu.make_async_copy(src, dst, ld_sem.at[i])
        for i, (src, dst) in enumerate(
            (
                (k_hbm, kw.at[0]),
                (v_hbm, vw.at[0]),
                (x_hbm, x_s),
                (chosen_hbm, chosen_s),
                (lse_hbm, lse_s.at[0]),
            )
        )
    )
    load_q, load_do = (
        [
            pltpu.make_async_copy(src.at[:, pl.ds(a * hd, hd)], dst.at[0, a], ld_sem.at[i])
            for a in range(heads)
        ]
        for i, src, dst in ((5, q_hbm, q6), (6, do_hbm, do6))
    )

    def all_of(ref, sem):
        return pltpu.make_async_copy(ref, ref, sem)

    for load in (load_k, load_chosen, *load_q, load_lse, load_v, *load_do, load_x):
        load.start()

    def remote(src, dst, send, recv, kv, t=None):
        return pltpu.make_async_remote_copy(
            src_ref=src,
            dst_ref=dst,
            send_sem=send,
            recv_sem=recv,
            device_id=(kv, tp if t is None else t),
            device_id_type=MESH,
        )

    def k_copy(d):
        return remote(kw.at[0], kw.at[d], kv_send, k_recv.at[d - 1], me + 2 * d)

    def v_copy(d):
        return remote(vw.at[0], vw.at[d], kv_send, v_recv, me + 2 * d)

    def dv_copy(d):
        return remote(dvo.at[d - 1], dvi.at[d - 1], back_send, dv_recv, me - 2 * d)

    def dk_copy(d):
        return remote(dko.at[d - 1], dki.at[d - 1], back_send, dk_recv, me - 2 * d)

    def each_count(left, wait):
        for count in range(1, BACK + 1):
            here = (left == count) if count < BACK else (left >= count)

            @pl.when(here)
            def _():
                wait(pl.ds(0, count))

    def to_sib(i, j, src, dst):
        return remote(src, dst, sib_send.at[i], sib_recv.at[j], sib)

    send_q = to_sib(0, 0, q6.at[0], q6.at[1])
    send_do = to_sib(0, 0, do6.at[0], do6.at[1])
    send_lse = to_sib(1, 1, lse_s.at[0], lse_s.at[1])
    send_bias = to_sib(2, 2, bias_out, bias_sib)
    send_x = to_sib(3, 3, x_t.at[:, 1 - core], x_in.at[tp, core])
    send_dl = to_sib(4, 4, dl_out, dl_in)
    send_dt = to_sib(4, 5, dt_out, dt_in)
    send_dq = [
        to_sib(5, 6 + i, dq_out.at[pl.ds(i * half_heads, half_heads)], dq_in.at[pl.ds(i * half_heads, half_heads)])
        for i in range(2)
    ]

    with scope("barrier_wait"):
        pl.semaphore_wait(barrier, count)

    def relay(point):
        for i, step, left, done in ((0, -BACK, ahead, behind), (1, BACK, behind, ahead)):
            hops = left // BACK
            turn = hops == point if point < LAST else hops >= point

            @pl.when(turn & (hops > 0))
            def _():
                pl.semaphore_wait(go_sem.at[i], 1)

            @pl.when(turn & (done >= BACK))
            def _():
                pl.semaphore_signal(
                    go_sem.at[i], inc=1, device_id=(me + 2 * step, tp), device_id_type=MESH
                )

    load_k.wait()
    for d in range(1, SPAN):

        @pl.when(chip + d < chips)
        def _():
            k_copy(d).start()

    relay(0)
    all_of(q6.at[0], ld_sem.at[5]).wait()
    send_q.start()
    load_lse.wait()
    send_lse.start()
    load_v.wait()
    for d in range(1, SPAN):

        @pl.when(chip + d < chips)
        def _():
            v_copy(d).start()

    load_chosen.wait()
    with scope("bias"):
        row = lax.broadcasted_iota(jnp.int32, (nblk, tok), 0)
        pos = lax.broadcasted_iota(jnp.int32, (1, tok), 1)
        lists = []
        for slot in range(chosen_s.shape[2]):
            ids = jnp.full((1, tok), NO_BLOCK, jnp.int32)
            for b in range(nblk):
                block = chosen_s[b, 0, slot]
                block = jnp.where(block < me * nblk + b, block, NO_BLOCK)
                ids = jnp.where(pos >= b * blk, block, ids)
            lists.append(ids)
        lists.append(me * nblk + pos // blk)
        for o in range(REACH + 1):
            ids = row + (me - o) * nblk
            hit = ids == lists[0]
            for other in lists[1:]:
                hit = hit | (ids == other)
            marked = jnp.where(hit, 0.0, MASKED)
            if o % 2:
                bias_out[o // 2] = marked
            else:
                bias_own[o // 2] = marked
        key_row = lax.broadcasted_iota(jnp.int32, (blk, tok), 0)
        query = lax.broadcasted_iota(jnp.int32, (blk, tok), 1)
        for j in range(nblk):
            own_bias[j * blk : (j + 1) * blk, :] = jnp.where(
                key_row + j * blk > query, MASKED, bias_own[0, j : j + 1, :]
            )
    all_of(do6.at[0], ld_sem.at[6]).wait()
    send_do.start()
    send_bias.start()

    load_x.wait()
    with scope("xT"):
        x_t[...] = x_s[...].T.reshape(x_t.shape)

    def end_rows(t):
        return pl.ds(lax.rem(t, 2) * half, half)

    early = end_rows(tp)
    x_copies = []
    for dt in range(1, nt):
        other = lax.rem(tp + dt, nt)
        for s, kv, par in ((0, me, core), (1, sib, 1 - core)):
            x_copies.append(
                remote(
                    x_t.at[early, par],
                    x_in.at[tp, core, early],
                    x_send.at[dt - 1],
                    x_recv.at[nt - dt - 1],
                    kv,
                    other,
                )
            )
    for copy in x_copies:
        copy.start()

    zero = jnp.zeros((tok, hd), bf)
    for d in range(1, SPAN):

        @pl.when(chip < d)
        def _():
            kw[d] = zero
            vw[d] = zero

        @pl.when(chip + d >= chips)
        def _():
            dvi[d - 1] = zero

    @pl.when(side == 1)
    def _():
        dki[0] = zero

    @pl.when(ahead < 2)
    def _():
        dki[1] = zero

    def weights(whose, slot, d, bias, buf):
        keys = kw[d]
        for a in range(heads):
            s = lax.dot_general(keys, q6[whose, a], NT, preferred_element_type=f32)
            s = s * (scale * LOG2E)
            lse = lse_s[whose, a : a + 1, :] * LOG2E
            if bias is None:
                p = jnp.exp2(s + (own_bias[...] - lse))
            else:
                p = jnp.exp2(s.reshape(nblk, blk, tok) + (bias - lse)[:, None, :]).reshape(tok, tok)
            p_s[a, slot] = p
            pb_s[buf, :, a * tok : (a + 1) * tok] = p.astype(bf)
        return jnp.dot(
            pb_s[buf], do6[whose].reshape(heads * tok, hd), preferred_element_type=f32
        )

    near = 1 - core
    far = 2 * core

    def far_tile():
        dv_far[...] = weights(1, SPAN + 1, far, bias_sib[core], 0)

    with scope("tile0"):
        dv_own[...] = weights(0, 0, 0, None, 0)

    with scope("q_wait"):
        all_of(q6, sib_recv.at[0]).wait()
        send_lse.wait_recv()
        send_bias.wait_recv()

    relay(1)

    @pl.when(core == 0)
    def _():
        with scope("far0"):
            far_tile()

    def tile1():
        with scope("k1_wait"):

            @pl.when(chip >= 1)
            def _():
                k_copy(1).wait_recv()

        with scope("d1"):
            dvo[0] = (
                weights(0, 1, 1, bias_own[1], 1) + weights(1, SPAN, 1, bias_sib[near], 0)
            ).astype(bf)

        @pl.when(chip >= 1)
        def _():
            dv_copy(1).start()

    def tile2():
        with scope("k2_wait"):

            @pl.when(chip >= 2)
            def _():
                k_copy(2).wait_recv()

        @pl.when(core == 1)
        def _():
            with scope("far1"):
                far_tile()

        with scope("d2"):
            dvo[1] = (
                weights(0, 2, 2, bias_own[2], 1) + jnp.where(core == 1, dv_far[...], 0.0)
            ).astype(bf)

        @pl.when(chip >= 2)
        def _():
            dv_copy(2).start()

    @pl.when(side == 0)
    def _():
        tile2()
        tile1()

    @pl.when(side == 1)
    def _():
        tile1()
        tile2()

    send_x.start()
    relay(2)
    for d in range(SPAN):
        kt[d] = kw[d].T

    with scope("v_wait"):
        each_count(behind, lambda rows: all_of(vw.at[rows], v_recv).wait())

    with scope("sib_gw"):
        for a in range(heads):
            total = jnp.zeros((1, tok), f32)
            for i, d in enumerate((1, far)):
                gw = lax.dot_general(vw[d], do6[1, a], NT, preferred_element_type=f32)
                t = p_s[a, SPAN + i] * gw
                t_s[a, i] = t
                total = total + jnp.sum(t, 0, keepdims=True)
            dl_out[a : a + 1, :] = total
    send_dl.start()

    with scope("dv_wait"):
        each_count(ahead, lambda rows: all_of(dvi.at[rows], dv_recv).wait())

    value = dv_own[...] + jnp.where(core == 0, dv_far[...], 0.0)
    for d in range(1, SPAN):
        value = value + dvi[d - 1].astype(f32)
    value = value.astype(bf)
    vg_ref[...] = value
    vall[tp * 2 + core] = value
    my_vg = vall.at[tp * 2 + core]
    vg_copies = [remote(my_vg, my_vg, vg_send, vg_recv.at[tp * 2 + core], sib)]
    for dt in range(1, nt):
        vg_copies.append(
            remote(my_vg, my_vg, vg_send, vg_recv.at[tp * 2 + core], me, lax.rem(tp + dt, nt))
        )
    for copy in vg_copies:
        copy.start()

    def score_grad(a):
        gw = lax.dot_general(
            vw[...].reshape(SPAN * tok, hd), do6[0, a], NT, preferred_element_type=f32
        )
        p = p_s[a, :SPAN].reshape(SPAN * tok, tok)
        own = jnp.sum(p * gw, 0, keepdims=True)
        dt_out[a : a + 1, :] = own
        delta = own + dl_in[a : a + 1, :]
        ds_own[:, a * tok : (a + 1) * tok] = (p * (gw - delta)).astype(bf)

    with scope("dl_wait"):
        send_dl.wait_recv()
    split = heads // 2
    with scope("own_ds_a"):
        for a in range(split):
            score_grad(a)

    def rs_copy(m):
        return remote(zo.at[m], ri.at[mine], rs_send, rs_recv, (2 * m + side) * 2 + core)

    def vg_wait(t, c):
        all_of(vall.at[t * 2 + c], vg_recv.at[t * 2 + c]).wait()

    def y_copy(g, first):
        rows = pl.ds(first // 2, hh)
        return remote(po.at[rows, 1 - side], yi.at[rows], y_send, y_recv.at[g], across)

    def put_rows(g, first, part):
        rows = pl.ds(first // 2, hh)
        pf[rows] = part.reshape(hh, 2, rw, hd)
        po[rows] = part.astype(bf).reshape(hh, 2, rw, hd)
        y_copy(g, first).start()

    def pass_rows(first):
        @pl.loop(0, hh)
        def _(j):
            @pl.when(first // 2 + j != mine)
            def _():
                rs_copy(first // 2 + j).start()

    def join_rows(g, first):
        with scope(f"y_wait{g}"):
            y_copy(g, first).wait_recv()
        rows = pl.ds(first // 2, hh)
        zo[rows] = (pf[rows, side] + yi[rows].astype(f32)).astype(bf)
        pass_rows(first)

    with scope("vg_wait"):
        vg_wait(tp, 1 - core)
        send_x.wait_recv()

    def own_rows(first, t):
        rows = pl.ds(first, half)
        return jnp.dot(
            x_t[rows, core].reshape(half * rw, tok), vall[t * 2 + core], preferred_element_type=f32
        ) + jnp.dot(
            x_in[tp, 1 - core, rows].reshape(half * rw, tok),
            vall[t * 2 + 1 - core],
            preferred_element_type=f32,
        )

    with scope("relay"):
        relay(LAST)
    groups = []
    with scope("w_end"):
        first = tp * per_tp + (1 - mid) * half
        put_rows(0, first, own_rows((1 - mid) * half, tp))
        groups.append((0, first))
    with scope("w_mid"):
        first = tp * per_tp + mid * half
        put_rows(nt, first, own_rows(mid * half, tp))
        groups.append((nt, first))

    with scope("own_ds_b"):
        for a in range(split, heads):
            score_grad(a)
    send_dt.start()

    def dk_part(ds, d, whose):
        return jnp.dot(
            ds[d * tok : (d + 1) * tok, :],
            q6[whose].reshape(heads * tok, hd),
            preferred_element_type=f32,
        )

    with scope("dk_own"):
        for d in range(1, SPAN):
            dk_acc[d - 1] = dk_part(ds_own, d, 0)

    for dt in range(1, nt):
        t = lax.rem(tp + dt, nt)
        rows = end_rows(t)
        with scope("x_wait"):
            all_of(x_in.at[t, :, rows], x_recv.at[dt - 1]).wait()
        with scope("w_early"):
            part = sum(
                jnp.dot(
                    x_in[t, c, rows].reshape(half * rw, tok),
                    vall[tp * 2 + c],
                    preferred_element_type=f32,
                )
                for c in range(2)
            )
            first = t * per_tp + lax.rem(t, 2) * half
            put_rows(dt, first, part)
            groups.append((dt, first))

    for dt in range(1, nt):
        i = lax.rem(tp + dt, nt) * 2 + core
        with scope("vg_x_wait"):
            all_of(vall.at[i], vg_recv.at[i]).wait()
        remote(vall.at[i], vall.at[i], vg_send, vg_recv.at[i], sib).start()

    with scope("dt_wait"):
        send_dt.wait_recv()
    with scope("sib_ds"):
        for a in range(heads):
            delta = dl_out[a : a + 1, :] + dt_in[a : a + 1, :]
            for i in range(2):
                ds_sib[i * tok : (i + 1) * tok, a * tok : (a + 1) * tok] = (
                    t_s[a, i] - p_s[a, SPAN + i] * delta
                ).astype(bf)
    with scope("dk_sib"):
        dko[0] = ((dk_acc[0] + dk_part(ds_sib, 0, 1)) * scale).astype(bf)
        dk_far = dk_part(ds_sib, 1, 1)
        dk_far2[...] = (dk_acc[1] + jnp.where(core == 1, dk_far, 0.0)) * scale
        dk_acc[0] = jnp.where(core == 0, dk_far, 0.0)
    merge = (side == 1) & (chip >= 3)
    hand = remote(dko.at[0], dk_pass, back_send, pass_recv, across)

    @pl.when(side == 1)
    def _():
        dk_copy(1).start()

    @pl.when((side == 0) & (chip >= 2))
    def _():
        hand.start()
        dko[1] = dk_far2[...].astype(bf)
        dk_copy(2).start()

    def merge_key():
        @pl.when(merge)
        def _():
            with scope("pass_wait"):
                hand.wait_recv()
            dko[1] = (dk_far2[...] + dk_pass[...].astype(f32)).astype(bf)
            dk_copy(2).start()

    def late_copy(dt, i):
        return remote(
            late.at[dt - 1, :, side if i == 0 else 1 - side],
            late_in.at[tp, side],
            late_send,
            late_recv.at[nt - dt - 1],
            me if i == 0 else across,
            lax.rem(tp + dt, nt),
        )

    for dt in range(1, nt):
        t = lax.rem(tp + dt, nt)
        with scope("vg_other_wait"):
            vg_wait(t, 1 - core)
        with scope("w_late"):
            late[dt - 1] = own_rows(mid * half, t).astype(bf).reshape(hh, 2, rw, hd)
            for i in (1, 0):
                late_copy(dt, i).start()

    def join_late():
        for dt in range(1, nt):
            t = lax.rem(tp + dt, nt)
            first = t * per_tp + (1 - lax.rem(t, 2)) * half
            with scope("late_wait"):
                all_of(late_in.at[t], late_recv.at[dt - 1]).wait()
            zo[pl.ds(first // 2, hh)] = (
                late_in[t, 0].astype(f32) + late_in[t, 1].astype(f32)
            ).astype(bf)
            pass_rows(first)

    def query_sib(i):
        with scope("dq_sib"):
            for a in range(i * split, (i + 1) * split):
                cols = pl.ds(a * tok, tok)
                dq = jnp.dot(kt[1], ds_sib[:tok, cols], preferred_element_type=f32) + jnp.dot(
                    kt[far], ds_sib[tok:, cols], preferred_element_type=f32
                )
                dq_out[a] = (dq * scale).astype(bf)
        send_dq[i].start()

    for group in groups[:2]:
        join_rows(*group)
    query_sib(0)
    query_sib(1)
    for group in groups[2:]:
        join_rows(*group)
    with scope("dk0"):
        key = (dk_acc[0] + dk_part(ds_own, 0, 0)) * scale
    merge_key()
    join_late()

    with scope("dq_own"):
        for i in range(2):
            send_dq[i].wait_recv()
            for a in range(i * split, (i + 1) * split):
                dq = sum(
                    jnp.dot(
                        kt[d],
                        ds_own[d * tok : (d + 1) * tok, a * tok : (a + 1) * tok],
                        preferred_element_type=f32,
                    )
                    for d in range(SPAN)
                )
                dq = dq * scale + dq_in[a].astype(f32)
                qg_ref[:, a * hd : (a + 1) * hd] = dq.T.astype(bf)

    with scope("dk_wait"):

        @pl.when((side == 0) & (ahead >= 2))
        def _():
            all_of(dki, dk_recv).wait()

        @pl.when((side == 0) != (ahead >= 2))
        def _():
            all_of(dki.at[0], dk_recv).wait()

    for d in range(BACK):
        key = key + dki[d].astype(f32)
    kg_ref[...] = key.astype(bf)

    with scope("rs_wait"):

        ri[pl.ds(mine, 1)] = zo[pl.ds(mine, 1)]
        all_of(ri.at[pl.ds(0, pairs - 1)], rs_recv).wait()
    wg_ref[...] = jnp.sum(ri[...].astype(f32), 0)

    with scope("send_wait"):
        each_count(ahead, lambda rows: all_of(kvw.at[:, rows], kv_send).wait())
        each_count(behind, lambda rows: all_of(back_out.at[:, rows], back_send).wait())
        all_of(q6, sib_send.at[0]).wait()
        send_lse.wait_send()
        send_bias.wait_send()
        send_x.wait_send()
        all_of(lse_s, sib_send.at[4]).wait()
        all_of(dq_out, sib_send.at[5]).wait()
        for dt in range(1, nt):
            all_of(x_t.at[early], x_send.at[dt - 1]).wait()
        all_of(vall.at[pl.ds(0, 2 * nt - 1)], vg_send).wait()
        all_of(late, late_send).wait()
        all_of(po.at[pl.ds(0, (nt + 1) * hh), 0], y_send).wait()
        all_of(ri.at[pl.ds(0, pairs - 1)], rs_send).wait()


def finish(*refs):
    count = len(refs) // 2
    sems = refs[-1]
    copies = [
        pltpu.make_async_copy(refs[i], refs[count + i], sems.at[i]) for i in range(count)
    ]
    for copy in copies:
        copy.start()
    for copy in copies:
        copy.wait()


def shards(nk, nt, queries, keys, values, log_sums, out_grad, chosen, inputs):
    tok, hd = keys.shape
    heads = queries.shape[1] // hd
    nblk = chosen.shape[0]
    feats = inputs.shape[1]
    rw = feats * nt // nk
    per_tp = feats // (2 * rw)
    bf, f32 = jnp.bfloat16, jnp.float32
    dma = pltpu.SemaphoreType.DMA
    vmem = pl.BlockSpec(memory_space=pltpu.VMEM)
    hbm = pl.BlockSpec(memory_space=pltpu.HBM)
    pairs = nk // 4
    parts = pl.pallas_call(
        functools.partial(kernel, nk, nt),
        out_shape=(
            pltpu.VMEM((tok, heads * hd), bf),
            pltpu.VMEM((tok, hd), bf),
            pltpu.VMEM((tok, hd), bf),
            pltpu.VMEM((rw, hd), f32),
        ),
        in_specs=[hbm] * 7,
        out_specs=(vmem, vmem, vmem, vmem),
        scratch_shapes=[
            pltpu.SMEM(chosen.shape, jnp.int32),
            pltpu.VMEM((2, heads, tok), f32),
            pltpu.VMEM((2, heads, tok, hd), bf),
            pltpu.VMEM((2, heads, tok, hd), bf),
            pltpu.VMEM((tok, feats), bf),
            pltpu.VMEM((2, SPAN, tok, hd), bf),
            pltpu.VMEM((SPAN, hd, tok), bf),
            pltpu.VMEM((SPAN, nblk, tok), f32),
            pltpu.VMEM((2, nblk, tok), f32),
            pltpu.VMEM((2, nblk, tok), f32),
            pltpu.VMEM((tok, tok), f32),
            pltpu.VMEM((heads, SPAN + 2, tok, tok), f32),
            pltpu.VMEM((heads, 2, tok, tok), f32),
            pltpu.VMEM((2, tok, heads * tok), bf),
            pltpu.VMEM((SPAN * tok, heads * tok), bf),
            pltpu.VMEM((2 * tok, heads * tok), bf),
            pltpu.VMEM((tok, hd), f32),
            pltpu.VMEM((tok, hd), f32),
            pltpu.VMEM((BACK, tok, hd), f32),
            pltpu.VMEM((2, BACK, tok, hd), bf),
            pltpu.VMEM((2, BACK, tok, hd), bf),
            pltpu.VMEM((tok, hd), bf),
            pltpu.VMEM((tok, hd), f32),
            pltpu.VMEM((heads, tok), f32),
            pltpu.VMEM((heads, tok), f32),
            pltpu.VMEM((heads, tok), f32),
            pltpu.VMEM((heads, tok), f32),
            pltpu.VMEM((heads, hd, tok), bf),
            pltpu.VMEM((heads, hd, tok), bf),
            pltpu.VMEM((per_tp, 2, rw, tok), bf),
            pltpu.VMEM((nt, 2, per_tp, rw, tok), bf),
            pltpu.VMEM((2 * nt, tok, hd), bf),
            pltpu.VMEM((nt - 1, per_tp // 4, 2, rw, hd), bf),
            pltpu.VMEM((nt, 2, per_tp // 4, rw, hd), bf),
            pltpu.VMEM((pairs, 2, rw, hd), f32),
            pltpu.VMEM((pairs, 2, rw, hd), bf),
            pltpu.VMEM((pairs, rw, hd), bf),
            pltpu.VMEM((pairs, rw, hd), bf),
            pltpu.VMEM((pairs, rw, hd), bf),
            dma((7,)),
            dma,
            dma((BACK,)),
            dma,
            dma,
            dma,
            dma,
            dma,
            dma((6,)),
            dma((8,)),
            dma((nt - 1,)),
            dma((nt - 1,)),
            dma,
            dma((2 * nt,)),
            dma,
            dma((nt - 1,)),
            dma,
            dma((nt + 1,)),
            dma,
            dma,
            pltpu.SemaphoreType.REGULAR((2,)),
        ],
        compiler_params=pltpu.CompilerParams(
            collective_id=0, has_side_effects=True, vmem_limit_bytes=60 * 1024 * 1024
        ),
    )(chosen, log_sums, keys, values, queries, out_grad, inputs)
    return pl.pallas_call(
        finish,
        out_shape=tuple(jax.ShapeDtypeStruct(part.shape, part.dtype) for part in parts),
        in_specs=[vmem] * len(parts),
        out_specs=(hbm,) * len(parts),
        scratch_shapes=[dma((len(parts),))],
    )(*(pltpu.with_memory_space_constraint(part, pltpu.VMEM) for part in parts))


def solution(mesh):
    in_specs = (
        P("kv", "tp"),
        P("kv", "tp"),
        P("kv", "tp"),
        P("tp", "kv"),
        P("kv", "tp"),
        P("kv", "tp", None),
        P("kv", "tp"),
    )
    out_specs = (P("kv", "tp"), P("kv", "tp"), P("kv", "tp"), P("kv", "tp"))
    return jax.shard_map(
        functools.partial(shards, mesh.shape["kv"], mesh.shape["tp"]),
        mesh=mesh,
        in_specs=in_specs,
        out_specs=out_specs,
        check_vma=False,
    )
```

```python
import functools

import jax
import jax.numpy as jnp
from jax import lax
from jax.experimental import pallas as pl
from jax.experimental.pallas import tpu as pltpu
from jax.sharding import PartitionSpec as P

REACH = 4
BACK = REACH // 2
SPAN = BACK + 1
STEPS = tuple(step for d in range(1, BACK + 1) for step in (d, -d))
LAST = 3
MASKED = -1e30
NO_BLOCK = -(1 << 20)
LOG2E = 1.4426950408889634
MESH = pl.DeviceIdType.MESH
NT = (((1,), (1,)), ((), ()))
scope = jax.named_scope


def kernel(
    nk,
    nt,
    chosen_hbm,
    lse_hbm,
    k_hbm,
    v_hbm,
    q_hbm,
    do_hbm,
    x_hbm,
    qg_ref,
    kg_ref,
    vg_ref,
    wg_ref,
    chosen_s,
    lse_s,
    q6,
    do6,
    x_s,
    kvw,
    kt,
    bias_own,
    bias_out,
    bias_sib,
    own_bias,
    p_s,
    t_s,
    pb_s,
    ds_own,
    ds_sib,
    dv_own,
    dv_far,
    dk_acc,
    back_out,
    back_in,
    dk_pass,
    dk_far2,
    dl_out,
    dl_in,
    dt_out,
    dt_in,
    dq_out,
    dq_in,
    x_t,
    x_in,
    vall,
    late,
    late_in,
    pf,
    po,
    yi,
    zo,
    ri,
    ld_sem,
    kv_send,
    k_recv,
    v_recv,
    back_send,
    dv_recv,
    dk_recv,
    pass_recv,
    sib_send,
    sib_recv,
    x_send,
    x_recv,
    vg_send,
    vg_recv,
    late_send,
    late_recv,
    y_send,
    y_recv,
    rs_send,
    rs_recv,
    go_sem,
):
    me = lax.axis_index("kv")
    tp = lax.axis_index("tp")
    core = lax.rem(me, 2)
    chip = me // 2
    sib = me + 1 - 2 * core
    side = lax.rem(chip, 2)
    across = me + 2 - 4 * side
    chips = nk // 2
    _, heads, tok, hd = q6.shape
    kw, vw = kvw.at[0], kvw.at[1]
    dvo, dko = back_out.at[0], back_out.at[1]
    dvi, dki = back_in.at[0], back_in.at[1]
    nblk = chosen_s.shape[0]
    blk = tok // nblk
    scale = hd**-0.5
    per_tp, _, rw, _ = x_t.shape
    half = per_tp // 2
    pairs = chips // 2
    hh = half // 2
    mine = chip // 2
    half_heads = heads // 2
    mid = 1 - lax.rem(tp, 2)
    f32, bf = jnp.float32, jnp.bfloat16

    behind = chip
    ahead = chips - 1 - chip
    near_chips = [(step, ahead >= step if step > 0 else behind >= -step) for step in STEPS]
    barrier = pltpu.get_barrier_semaphore()
    count = 1 + 3 * (nt - 1)
    for step, exists in near_chips:
        count = count + jnp.where(exists, 1, 0)

        @pl.when(exists)
        def _():
            pl.semaphore_signal(
                barrier, inc=1, device_id=(me + 2 * step, tp), device_id_type=MESH
            )

    pl.semaphore_signal(barrier, inc=1, device_id=(sib, tp), device_id_type=MESH)
    for dt in range(1, nt):
        for kv in (me, sib, across):
            pl.semaphore_signal(
                barrier, inc=1, device_id=(kv, lax.rem(tp + dt, nt)), device_id_type=MESH
            )

    load_k, load_v, load_x, load_chosen, load_lse = (
        pltpu.make_async_copy(src, dst, ld_sem.at[i])
        for i, (src, dst) in enumerate(
            (
                (k_hbm, kw.at[0]),
                (v_hbm, vw.at[0]),
                (x_hbm, x_s),
                (chosen_hbm, chosen_s),
                (lse_hbm, lse_s.at[0]),
            )
        )
    )
    load_q, load_do = (
        [
            pltpu.make_async_copy(src.at[:, pl.ds(a * hd, hd)], dst.at[0, a], ld_sem.at[i])
            for a in range(heads)
        ]
        for i, src, dst in ((5, q_hbm, q6), (6, do_hbm, do6))
    )

    def all_of(ref, sem):
        return pltpu.make_async_copy(ref, ref, sem)

    for load in (load_k, load_chosen, *load_q, load_lse, load_v, *load_do, load_x):
        load.start()

    def remote(src, dst, send, recv, kv, t=None):
        return pltpu.make_async_remote_copy(
            src_ref=src,
            dst_ref=dst,
            send_sem=send,
            recv_sem=recv,
            device_id=(kv, tp if t is None else t),
            device_id_type=MESH,
        )

    def k_copy(d):
        return remote(kw.at[0], kw.at[d], kv_send, k_recv.at[d - 1], me + 2 * d)

    def v_copy(d):
        return remote(vw.at[0], vw.at[d], kv_send, v_recv, me + 2 * d)

    def dv_copy(d):
        return remote(dvo.at[d - 1], dvi.at[d - 1], back_send, dv_recv, me - 2 * d)

    def dk_copy(d):
        return remote(dko.at[d - 1], dki.at[d - 1], back_send, dk_recv, me - 2 * d)

    def each_count(left, wait):
        for count in range(1, BACK + 1):
            here = (left == count) if count < BACK else (left >= count)

            @pl.when(here)
            def _():
                wait(pl.ds(0, count))

    def to_sib(i, j, src, dst):
        return remote(src, dst, sib_send.at[i], sib_recv.at[j], sib)

    send_q = to_sib(0, 0, q6.at[0], q6.at[1])
    send_do = to_sib(0, 0, do6.at[0], do6.at[1])
    send_lse = to_sib(1, 1, lse_s.at[0], lse_s.at[1])
    send_bias = to_sib(2, 2, bias_out, bias_sib)
    send_x = to_sib(3, 3, x_t.at[:, 1 - core], x_in.at[tp, core])
    send_dl = to_sib(4, 4, dl_out, dl_in)
    send_dt = to_sib(4, 5, dt_out, dt_in)
    send_dq = [
        to_sib(5, 6 + i, dq_out.at[pl.ds(i * half_heads, half_heads)], dq_in.at[pl.ds(i * half_heads, half_heads)])
        for i in range(2)
    ]

    with scope("barrier_wait"):
        pl.semaphore_wait(barrier, count)

    def relay(point):
        for i, step, left, done in ((0, -BACK, ahead, behind), (1, BACK, behind, ahead)):
            hops = left // BACK
            turn = hops == point if point < LAST else hops >= point

            @pl.when(turn & (hops > 0))
            def _():
                pl.semaphore_wait(go_sem.at[i], 1)

            @pl.when(turn & (done >= BACK))
            def _():
                pl.semaphore_signal(
                    go_sem.at[i], inc=1, device_id=(me + 2 * step, tp), device_id_type=MESH
                )

    load_k.wait()
    for d in range(1, SPAN):

        @pl.when(chip + d < chips)
        def _():
            k_copy(d).start()

    relay(0)
    all_of(q6.at[0], ld_sem.at[5]).wait()
    send_q.start()
    load_lse.wait()
    send_lse.start()
    load_v.wait()
    for d in range(1, SPAN):

        @pl.when(chip + d < chips)
        def _():
            v_copy(d).start()

    load_chosen.wait()
    with scope("bias"):
        row = lax.broadcasted_iota(jnp.int32, (nblk, tok), 0)
        pos = lax.broadcasted_iota(jnp.int32, (1, tok), 1)
        lists = []
        for slot in range(chosen_s.shape[2]):
            ids = jnp.full((1, tok), NO_BLOCK, jnp.int32)
            for b in range(nblk):
                block = chosen_s[b, 0, slot]
                block = jnp.where(block < me * nblk + b, block, NO_BLOCK)
                ids = jnp.where(pos >= b * blk, block, ids)
            lists.append(ids)
        lists.append(me * nblk + pos // blk)
        for o in range(REACH + 1):
            ids = row + (me - o) * nblk
            hit = ids == lists[0]
            for other in lists[1:]:
                hit = hit | (ids == other)
            marked = jnp.where(hit, 0.0, MASKED)
            if o % 2:
                bias_out[o // 2] = marked
            else:
                bias_own[o // 2] = marked
        key_row = lax.broadcasted_iota(jnp.int32, (blk, tok), 0)
        query = lax.broadcasted_iota(jnp.int32, (blk, tok), 1)
        for j in range(nblk):
            own_bias[j * blk : (j + 1) * blk, :] = jnp.where(
                key_row + j * blk > query, MASKED, bias_own[0, j : j + 1, :]
            )
    all_of(do6.at[0], ld_sem.at[6]).wait()
    send_do.start()
    send_bias.start()

    load_x.wait()
    with scope("xT"):
        x_t[...] = x_s[...].T.reshape(x_t.shape)

    def end_rows(t):
        return pl.ds(lax.rem(t, 2) * half, half)

    early = end_rows(tp)
    x_copies = []
    for dt in range(1, nt):
        other = lax.rem(tp + dt, nt)
        for s, kv, par in ((0, me, core), (1, sib, 1 - core)):
            x_copies.append(
                remote(
                    x_t.at[early, par],
                    x_in.at[tp, core, early],
                    x_send.at[dt - 1],
                    x_recv.at[nt - dt - 1],
                    kv,
                    other,
                )
            )
    for copy in x_copies:
        copy.start()

    zero = jnp.zeros((tok, hd), bf)
    for d in range(1, SPAN):

        @pl.when(chip < d)
        def _():
            kw[d] = zero
            vw[d] = zero

        @pl.when(chip + d >= chips)
        def _():
            dvi[d - 1] = zero

    @pl.when(side == 1)
    def _():
        dki[0] = zero

    @pl.when(ahead < 2)
    def _():
        dki[1] = zero

    def weights(whose, slot, d, bias, buf):
        keys = kw[d]
        for a in range(heads):
            s = lax.dot_general(keys, q6[whose, a], NT, preferred_element_type=f32)
            s = s * (scale * LOG2E)
            lse = lse_s[whose, a : a + 1, :] * LOG2E
            if bias is None:
                p = jnp.exp2(s + (own_bias[...] - lse))
            else:
                p = jnp.exp2(s.reshape(nblk, blk, tok) + (bias - lse)[:, None, :]).reshape(tok, tok)
            p_s[a, slot] = p
            pb_s[buf, :, a * tok : (a + 1) * tok] = p.astype(bf)
        return jnp.dot(
            pb_s[buf], do6[whose].reshape(heads * tok, hd), preferred_element_type=f32
        )

    near = 1 - core
    far = 2 * core

    def far_tile():
        dv_far[...] = weights(1, SPAN + 1, far, bias_sib[core], 0)

    with scope("tile0"):
        dv_own[...] = weights(0, 0, 0, None, 0)

    with scope("q_wait"):
        all_of(q6, sib_recv.at[0]).wait()
        send_lse.wait_recv()
        send_bias.wait_recv()

    relay(1)

    @pl.when(core == 0)
    def _():
        with scope("far0"):
            far_tile()

    def tile1():
        with scope("k1_wait"):

            @pl.when(chip >= 1)
            def _():
                k_copy(1).wait_recv()

        with scope("d1"):
            dvo[0] = (
                weights(0, 1, 1, bias_own[1], 1) + weights(1, SPAN, 1, bias_sib[near], 0)
            ).astype(bf)

        @pl.when(chip >= 1)
        def _():
            dv_copy(1).start()

    def tile2():
        with scope("k2_wait"):

            @pl.when(chip >= 2)
            def _():
                k_copy(2).wait_recv()

        @pl.when(core == 1)
        def _():
            with scope("far1"):
                far_tile()

        with scope("d2"):
            dvo[1] = (
                weights(0, 2, 2, bias_own[2], 1) + jnp.where(core == 1, dv_far[...], 0.0)
            ).astype(bf)

        @pl.when(chip >= 2)
        def _():
            dv_copy(2).start()

    @pl.when(side == 0)
    def _():
        tile2()
        tile1()

    @pl.when(side == 1)
    def _():
        tile1()
        tile2()

    send_x.start()
    relay(2)
    for d in range(SPAN):
        kt[d] = kw[d].T

    with scope("v_wait"):
        each_count(behind, lambda rows: all_of(vw.at[rows], v_recv).wait())

    with scope("sib_gw"):
        for a in range(heads):
            total = jnp.zeros((1, tok), f32)
            for i, d in enumerate((1, far)):
                gw = lax.dot_general(vw[d], do6[1, a], NT, preferred_element_type=f32)
                t = p_s[a, SPAN + i] * gw
                t_s[a, i] = t
                total = total + jnp.sum(t, 0, keepdims=True)
            dl_out[a : a + 1, :] = total
    send_dl.start()

    with scope("dv_wait"):
        each_count(ahead, lambda rows: all_of(dvi.at[rows], dv_recv).wait())

    value = dv_own[...] + jnp.where(core == 0, dv_far[...], 0.0)
    for d in range(1, SPAN):
        value = value + dvi[d - 1].astype(f32)
    value = value.astype(bf)
    vg_ref[...] = value
    vall[tp * 2 + core] = value
    my_vg = vall.at[tp * 2 + core]
    vg_copies = [remote(my_vg, my_vg, vg_send, vg_recv.at[tp * 2 + core], sib)]
    for dt in range(1, nt):
        vg_copies.append(
            remote(my_vg, my_vg, vg_send, vg_recv.at[tp * 2 + core], me, lax.rem(tp + dt, nt))
        )
    for copy in vg_copies:
        copy.start()

    def score_grad(a):
        gw = lax.dot_general(
            vw[...].reshape(SPAN * tok, hd), do6[0, a], NT, preferred_element_type=f32
        )
        p = p_s[a, :SPAN].reshape(SPAN * tok, tok)
        own = jnp.sum(p * gw, 0, keepdims=True)
        dt_out[a : a + 1, :] = own
        delta = own + dl_in[a : a + 1, :]
        ds_own[:, a * tok : (a + 1) * tok] = (p * (gw - delta)).astype(bf)

    with scope("dl_wait"):
        send_dl.wait_recv()
    split = heads // 2
    with scope("own_ds_a"):
        for a in range(split):
            score_grad(a)

    def rs_copy(m):
        return remote(zo.at[m], ri.at[mine], rs_send, rs_recv, (2 * m + side) * 2 + core)

    def vg_wait(t, c):
        all_of(vall.at[t * 2 + c], vg_recv.at[t * 2 + c]).wait()

    def y_copy(g, first):
        rows = pl.ds(first // 2, hh)
        return remote(po.at[rows, 1 - side], yi.at[rows], y_send, y_recv.at[g], across)

    def put_rows(g, first, part):
        rows = pl.ds(first // 2, hh)
        pf[rows] = part.reshape(hh, 2, rw, hd)
        po[rows] = part.astype(bf).reshape(hh, 2, rw, hd)
        y_copy(g, first).start()

    def pass_rows(first):
        @pl.loop(0, hh)
        def _(j):
            @pl.when(first // 2 + j != mine)
            def _():
                rs_copy(first // 2 + j).start()

    def join_rows(g, first):
        with scope(f"y_wait{g}"):
            y_copy(g, first).wait_recv()
        rows = pl.ds(first // 2, hh)
        zo[rows] = (pf[rows, side] + yi[rows].astype(f32)).astype(bf)
        pass_rows(first)

    with scope("vg_wait"):
        vg_wait(tp, 1 - core)
        send_x.wait_recv()

    def own_rows(first, t):
        rows = pl.ds(first, half)
        return jnp.dot(
            x_t[rows, core].reshape(half * rw, tok), vall[t * 2 + core], preferred_element_type=f32
        ) + jnp.dot(
            x_in[tp, 1 - core, rows].reshape(half * rw, tok),
            vall[t * 2 + 1 - core],
            preferred_element_type=f32,
        )

    with scope("relay"):
        relay(LAST)
    groups = []
    with scope("w_end"):
        first = tp * per_tp + (1 - mid) * half
        put_rows(0, first, own_rows((1 - mid) * half, tp))
        groups.append((0, first))
    with scope("w_mid"):
        first = tp * per_tp + mid * half
        put_rows(nt, first, own_rows(mid * half, tp))
        groups.append((nt, first))

    with scope("own_ds_b"):
        for a in range(split, heads):
            score_grad(a)
    send_dt.start()

    def dk_part(ds, d, whose):
        return jnp.dot(
            ds[d * tok : (d + 1) * tok, :],
            q6[whose].reshape(heads * tok, hd),
            preferred_element_type=f32,
        )

    with scope("dk_own"):
        for d in range(1, SPAN):
            dk_acc[d - 1] = dk_part(ds_own, d, 0)

    for dt in range(1, nt):
        t = lax.rem(tp + dt, nt)
        rows = end_rows(t)
        with scope("x_wait"):
            all_of(x_in.at[t, :, rows], x_recv.at[dt - 1]).wait()
        with scope("w_early"):
            part = sum(
                jnp.dot(
                    x_in[t, c, rows].reshape(half * rw, tok),
                    vall[tp * 2 + c],
                    preferred_element_type=f32,
                )
                for c in range(2)
            )
            first = t * per_tp + lax.rem(t, 2) * half
            put_rows(dt, first, part)
            groups.append((dt, first))

    for dt in range(1, nt):
        i = lax.rem(tp + dt, nt) * 2 + core
        with scope("vg_x_wait"):
            all_of(vall.at[i], vg_recv.at[i]).wait()
        remote(vall.at[i], vall.at[i], vg_send, vg_recv.at[i], sib).start()

    with scope("dt_wait"):
        send_dt.wait_recv()
    with scope("sib_ds"):
        for a in range(heads):
            delta = dl_out[a : a + 1, :] + dt_in[a : a + 1, :]
            for i in range(2):
                ds_sib[i * tok : (i + 1) * tok, a * tok : (a + 1) * tok] = (
                    t_s[a, i] - p_s[a, SPAN + i] * delta
                ).astype(bf)
    with scope("dk_sib"):
        dko[0] = ((dk_acc[0] + dk_part(ds_sib, 0, 1)) * scale).astype(bf)
        dk_far = dk_part(ds_sib, 1, 1)
        dk_far2[...] = (dk_acc[1] + jnp.where(core == 1, dk_far, 0.0)) * scale
        dk_acc[0] = jnp.where(core == 0, dk_far, 0.0)
    merge = (side == 1) & (chip >= 3)
    hand = remote(dko.at[0], dk_pass, back_send, pass_recv, across)

    @pl.when(side == 1)
    def _():
        dk_copy(1).start()

    @pl.when((side == 0) & (chip >= 2))
    def _():
        hand.start()
        dko[1] = dk_far2[...].astype(bf)
        dk_copy(2).start()

    def merge_key():
        @pl.when(merge)
        def _():
            with scope("pass_wait"):
                hand.wait_recv()
            dko[1] = (dk_far2[...] + dk_pass[...].astype(f32)).astype(bf)
            dk_copy(2).start()

    def late_copy(dt, i):
        return remote(
            late.at[dt - 1, :, side if i == 0 else 1 - side],
            late_in.at[tp, side],
            late_send,
            late_recv.at[nt - dt - 1],
            me if i == 0 else across,
            lax.rem(tp + dt, nt),
        )

    for dt in range(1, nt):
        t = lax.rem(tp + dt, nt)
        with scope("vg_other_wait"):
            vg_wait(t, 1 - core)
        with scope("w_late"):
            late[dt - 1] = own_rows(mid * half, t).astype(bf).reshape(hh, 2, rw, hd)
            for i in (1, 0):
                late_copy(dt, i).start()

    def join_late():
        for dt in range(1, nt):
            t = lax.rem(tp + dt, nt)
            first = t * per_tp + (1 - lax.rem(t, 2)) * half
            with scope("late_wait"):
                all_of(late_in.at[t], late_recv.at[dt - 1]).wait()
            zo[pl.ds(first // 2, hh)] = (
                late_in[t, 0].astype(f32) + late_in[t, 1].astype(f32)
            ).astype(bf)
            pass_rows(first)

    def query_sib(i):
        with scope("dq_sib"):
            for a in range(i * split, (i + 1) * split):
                cols = pl.ds(a * tok, tok)
                dq = jnp.dot(kt[1], ds_sib[:tok, cols], preferred_element_type=f32) + jnp.dot(
                    kt[far], ds_sib[tok:, cols], preferred_element_type=f32
                )
                dq_out[a] = (dq * scale).astype(bf)
        send_dq[i].start()

    join_rows(*groups[0])
    query_sib(0)
    for group in groups[2:]:
        join_rows(*group)
    join_rows(*groups[1])
    query_sib(1)
    with scope("dk0"):
        key = (dk_acc[0] + dk_part(ds_own, 0, 0)) * scale
    merge_key()
    join_late()

    with scope("dq_own"):
        for i in range(2):
            send_dq[i].wait_recv()
            for a in range(i * split, (i + 1) * split):
                dq = sum(
                    jnp.dot(
                        kt[d],
                        ds_own[d * tok : (d + 1) * tok, a * tok : (a + 1) * tok],
                        preferred_element_type=f32,
                    )
                    for d in range(SPAN)
                )
                dq = dq * scale + dq_in[a].astype(f32)
                qg_ref[:, a * hd : (a + 1) * hd] = dq.T.astype(bf)

    with scope("dk_wait"):

        @pl.when((side == 0) & (ahead >= 2))
        def _():
            all_of(dki, dk_recv).wait()

        @pl.when((side == 0) != (ahead >= 2))
        def _():
            all_of(dki.at[0], dk_recv).wait()

    for d in range(BACK):
        key = key + dki[d].astype(f32)
    kg_ref[...] = key.astype(bf)

    with scope("rs_wait"):

        ri[pl.ds(mine, 1)] = zo[pl.ds(mine, 1)]
        all_of(ri.at[pl.ds(0, pairs - 1)], rs_recv).wait()
    wg_ref[...] = jnp.sum(ri[...].astype(f32), 0)

    with scope("send_wait"):
        each_count(ahead, lambda rows: all_of(kvw.at[:, rows], kv_send).wait())
        each_count(behind, lambda rows: all_of(back_out.at[:, rows], back_send).wait())
        all_of(q6, sib_send.at[0]).wait()
        send_lse.wait_send()
        send_bias.wait_send()
        send_x.wait_send()
        all_of(lse_s, sib_send.at[4]).wait()
        all_of(dq_out, sib_send.at[5]).wait()
        for dt in range(1, nt):
            all_of(x_t.at[early], x_send.at[dt - 1]).wait()
        all_of(vall.at[pl.ds(0, 2 * nt - 1)], vg_send).wait()
        all_of(late, late_send).wait()
        all_of(po.at[pl.ds(0, (nt + 1) * hh), 0], y_send).wait()
        all_of(ri.at[pl.ds(0, pairs - 1)], rs_send).wait()


def finish(*refs):
    count = len(refs) // 2
    sems = refs[-1]
    copies = [
        pltpu.make_async_copy(refs[i], refs[count + i], sems.at[i]) for i in range(count)
    ]
    for copy in copies:
        copy.start()
    for copy in copies:
        copy.wait()


def shards(nk, nt, queries, keys, values, log_sums, out_grad, chosen, inputs):
    tok, hd = keys.shape
    heads = queries.shape[1] // hd
    nblk = chosen.shape[0]
    feats = inputs.shape[1]
    rw = feats * nt // nk
    per_tp = feats // (2 * rw)
    bf, f32 = jnp.bfloat16, jnp.float32
    dma = pltpu.SemaphoreType.DMA
    vmem = pl.BlockSpec(memory_space=pltpu.VMEM)
    hbm = pl.BlockSpec(memory_space=pltpu.HBM)
    pairs = nk // 4
    parts = pl.pallas_call(
        functools.partial(kernel, nk, nt),
        out_shape=(
            pltpu.VMEM((tok, heads * hd), bf),
            pltpu.VMEM((tok, hd), bf),
            pltpu.VMEM((tok, hd), bf),
            pltpu.VMEM((rw, hd), f32),
        ),
        in_specs=[hbm] * 7,
        out_specs=(vmem, vmem, vmem, vmem),
        scratch_shapes=[
            pltpu.SMEM(chosen.shape, jnp.int32),
            pltpu.VMEM((2, heads, tok), f32),
            pltpu.VMEM((2, heads, tok, hd), bf),
            pltpu.VMEM((2, heads, tok, hd), bf),
            pltpu.VMEM((tok, feats), bf),
            pltpu.VMEM((2, SPAN, tok, hd), bf),
            pltpu.VMEM((SPAN, hd, tok), bf),
            pltpu.VMEM((SPAN, nblk, tok), f32),
            pltpu.VMEM((2, nblk, tok), f32),
            pltpu.VMEM((2, nblk, tok), f32),
            pltpu.VMEM((tok, tok), f32),
            pltpu.VMEM((heads, SPAN + 2, tok, tok), f32),
            pltpu.VMEM((heads, 2, tok, tok), f32),
            pltpu.VMEM((2, tok, heads * tok), bf),
            pltpu.VMEM((SPAN * tok, heads * tok), bf),
            pltpu.VMEM((2 * tok, heads * tok), bf),
            pltpu.VMEM((tok, hd), f32),
            pltpu.VMEM((tok, hd), f32),
            pltpu.VMEM((BACK, tok, hd), f32),
            pltpu.VMEM((2, BACK, tok, hd), bf),
            pltpu.VMEM((2, BACK, tok, hd), bf),
            pltpu.VMEM((tok, hd), bf),
            pltpu.VMEM((tok, hd), f32),
            pltpu.VMEM((heads, tok), f32),
            pltpu.VMEM((heads, tok), f32),
            pltpu.VMEM((heads, tok), f32),
            pltpu.VMEM((heads, tok), f32),
            pltpu.VMEM((heads, hd, tok), bf),
            pltpu.VMEM((heads, hd, tok), bf),
            pltpu.VMEM((per_tp, 2, rw, tok), bf),
            pltpu.VMEM((nt, 2, per_tp, rw, tok), bf),
            pltpu.VMEM((2 * nt, tok, hd), bf),
            pltpu.VMEM((nt - 1, per_tp // 4, 2, rw, hd), bf),
            pltpu.VMEM((nt, 2, per_tp // 4, rw, hd), bf),
            pltpu.VMEM((pairs, 2, rw, hd), f32),
            pltpu.VMEM((pairs, 2, rw, hd), bf),
            pltpu.VMEM((pairs, rw, hd), bf),
            pltpu.VMEM((pairs, rw, hd), bf),
            pltpu.VMEM((pairs, rw, hd), bf),
            dma((7,)),
            dma,
            dma((BACK,)),
            dma,
            dma,
            dma,
            dma,
            dma,
            dma((6,)),
            dma((8,)),
            dma((nt - 1,)),
            dma((nt - 1,)),
            dma,
            dma((2 * nt,)),
            dma,
            dma((nt - 1,)),
            dma,
            dma((nt + 1,)),
            dma,
            dma,
            pltpu.SemaphoreType.REGULAR((2,)),
        ],
        compiler_params=pltpu.CompilerParams(
            collective_id=0, has_side_effects=True, vmem_limit_bytes=60 * 1024 * 1024
        ),
    )(chosen, log_sums, keys, values, queries, out_grad, inputs)
    return pl.pallas_call(
        finish,
        out_shape=tuple(jax.ShapeDtypeStruct(part.shape, part.dtype) for part in parts),
        in_specs=[vmem] * len(parts),
        out_specs=(hbm,) * len(parts),
        scratch_shapes=[dma((len(parts),))],
    )(*(pltpu.with_memory_space_constraint(part, pltpu.VMEM) for part in parts))


def solution(mesh):
    in_specs = (
        P("kv", "tp"),
        P("kv", "tp"),
        P("kv", "tp"),
        P("tp", "kv"),
        P("kv", "tp"),
        P("kv", "tp", None),
        P("kv", "tp"),
    )
    out_specs = (P("kv", "tp"), P("kv", "tp"), P("kv", "tp"), P("kv", "tp"))
    return jax.shard_map(
        functools.partial(shards, mesh.shape["kv"], mesh.shape["tp"]),
        mesh=mesh,
        in_specs=in_specs,
        out_specs=out_specs,
        check_vma=False,
    )
```

```python
import functools

import jax
import jax.numpy as jnp
from jax import lax
from jax.experimental import pallas as pl
from jax.experimental.pallas import tpu as pltpu
from jax.sharding import PartitionSpec as P

REACH = 4
BACK = REACH // 2
SPAN = BACK + 1
STEPS = tuple(step for d in range(1, BACK + 1) for step in (d, -d))
LAST = 3
MASKED = -1e30
NO_BLOCK = -(1 << 20)
LOG2E = 1.4426950408889634
MESH = pl.DeviceIdType.MESH
NT = (((1,), (1,)), ((), ()))
scope = jax.named_scope


def kernel(
    nk,
    nt,
    chosen_hbm,
    lse_hbm,
    k_hbm,
    v_hbm,
    q_hbm,
    do_hbm,
    x_hbm,
    qg_ref,
    kg_ref,
    vg_ref,
    wg_ref,
    chosen_s,
    lse_s,
    q6,
    do6,
    x_s,
    kvw,
    kt,
    bias_own,
    bias_out,
    bias_sib,
    own_bias,
    p_s,
    t_s,
    pb_s,
    ds_own,
    ds_sib,
    dv_own,
    dv_far,
    dk_acc,
    back_out,
    back_in,
    dk_pass,
    dk_far2,
    dl_out,
    dl_in,
    dt_out,
    dt_in,
    dq_out,
    dq_in,
    x_t,
    x_in,
    vall,
    late,
    late_in,
    pf,
    po,
    yi,
    zo,
    ri,
    ld_sem,
    kv_send,
    k_recv,
    v_recv,
    back_send,
    dv_recv,
    dk_recv,
    pass_recv,
    sib_send,
    sib_recv,
    x_send,
    x_recv,
    vg_send,
    vg_recv,
    late_send,
    late_recv,
    y_send,
    y_recv,
    rs_send,
    rs_recv,
    go_sem,
):
    me = lax.axis_index("kv")
    tp = lax.axis_index("tp")
    core = lax.rem(me, 2)
    chip = me // 2
    sib = me + 1 - 2 * core
    side = lax.rem(chip, 2)
    across = me + 2 - 4 * side
    chips = nk // 2
    _, heads, tok, hd = q6.shape
    kw, vw = kvw.at[0], kvw.at[1]
    dvo, dko = back_out.at[0], back_out.at[1]
    dvi, dki = back_in.at[0], back_in.at[1]
    nblk = chosen_s.shape[0]
    blk = tok // nblk
    scale = hd**-0.5
    per_tp, _, rw, _ = x_t.shape
    half = per_tp // 2
    pairs = chips // 2
    hh = half // 2
    mine = chip // 2
    half_heads = heads // 2
    mid = 1 - lax.rem(tp, 2)
    f32, bf = jnp.float32, jnp.bfloat16

    behind = chip
    ahead = chips - 1 - chip
    near_chips = [(step, ahead >= step if step > 0 else behind >= -step) for step in STEPS]
    barrier = pltpu.get_barrier_semaphore()
    count = 1 + 2 * (nt - 1)
    for step, exists in near_chips:
        count = count + jnp.where(exists, 1, 0)

        @pl.when(exists)
        def _():
            pl.semaphore_signal(
                barrier, inc=1, device_id=(me + 2 * step, tp), device_id_type=MESH
            )

    pl.semaphore_signal(barrier, inc=1, device_id=(sib, tp), device_id_type=MESH)
    for dt in range(1, nt):
        for kv in (me, sib):
            pl.semaphore_signal(
                barrier, inc=1, device_id=(kv, lax.rem(tp + dt, nt)), device_id_type=MESH
            )

    load_k, load_v, load_x, load_chosen, load_lse = (
        pltpu.make_async_copy(src, dst, ld_sem.at[i])
        for i, (src, dst) in enumerate(
            (
                (k_hbm, kw.at[0]),
                (v_hbm, vw.at[0]),
                (x_hbm, x_s),
                (chosen_hbm, chosen_s),
                (lse_hbm, lse_s.at[0]),
            )
        )
    )
    load_q, load_do = (
        [
            pltpu.make_async_copy(src.at[:, pl.ds(a * hd, hd)], dst.at[0, a], ld_sem.at[i])
            for a in range(heads)
        ]
        for i, src, dst in ((5, q_hbm, q6), (6, do_hbm, do6))
    )

    def all_of(ref, sem):
        return pltpu.make_async_copy(ref, ref, sem)

    for load in (load_k, load_chosen, *load_q, load_lse, load_v, *load_do, load_x):
        load.start()

    def remote(src, dst, send, recv, kv, t=None):
        return pltpu.make_async_remote_copy(
            src_ref=src,
            dst_ref=dst,
            send_sem=send,
            recv_sem=recv,
            device_id=(kv, tp if t is None else t),
            device_id_type=MESH,
        )

    def k_copy(d):
        return remote(kw.at[0], kw.at[d], kv_send, k_recv.at[d - 1], me + 2 * d)

    def v_copy(d):
        return remote(vw.at[0], vw.at[d], kv_send, v_recv, me + 2 * d)

    def dv_copy(d):
        return remote(dvo.at[d - 1], dvi.at[d - 1], back_send, dv_recv, me - 2 * d)

    def dk_copy(d):
        return remote(dko.at[d - 1], dki.at[d - 1], back_send, dk_recv, me - 2 * d)

    def each_count(left, wait):
        for count in range(1, BACK + 1):
            here = (left == count) if count < BACK else (left >= count)

            @pl.when(here)
            def _():
                wait(pl.ds(0, count))

    def to_sib(i, j, src, dst):
        return remote(src, dst, sib_send.at[i], sib_recv.at[j], sib)

    send_q = to_sib(0, 0, q6.at[0], q6.at[1])
    send_do = to_sib(0, 0, do6.at[0], do6.at[1])
    send_lse = to_sib(1, 1, lse_s.at[0], lse_s.at[1])
    send_bias = to_sib(2, 2, bias_out, bias_sib)
    send_x = to_sib(3, 3, x_t.at[:, 1 - core], x_in.at[tp, core])
    send_dl = to_sib(4, 4, dl_out, dl_in)
    send_dt = to_sib(4, 5, dt_out, dt_in)
    send_dq = [
        to_sib(5, 6 + i, dq_out.at[pl.ds(i * half_heads, half_heads)], dq_in.at[pl.ds(i * half_heads, half_heads)])
        for i in range(2)
    ]

    with scope("barrier_wait"):
        pl.semaphore_wait(barrier, count)
    for dt in range(1, nt):
        pl.semaphore_signal(
            go_sem.at[2], inc=1, device_id=(me, lax.rem(tp + dt, nt)), device_id_type=MESH
        )

    def relay(point):
        for i, step, left, done in ((0, -BACK, ahead, behind), (1, BACK, behind, ahead)):
            hops = left // BACK
            turn = hops == point if point < LAST else hops >= point

            @pl.when(turn & (hops > 0))
            def _():
                pl.semaphore_wait(go_sem.at[i], 1)

            @pl.when(turn & (done >= BACK))
            def _():
                pl.semaphore_signal(
                    go_sem.at[i], inc=1, device_id=(me + 2 * step, tp), device_id_type=MESH
                )

    load_k.wait()
    for d in range(1, SPAN):

        @pl.when(chip + d < chips)
        def _():
            k_copy(d).start()

    relay(0)
    all_of(q6.at[0], ld_sem.at[5]).wait()
    send_q.start()
    load_lse.wait()
    send_lse.start()
    load_v.wait()
    for d in range(1, SPAN):

        @pl.when(chip + d < chips)
        def _():
            v_copy(d).start()

    load_chosen.wait()
    with scope("bias"):
        row = lax.broadcasted_iota(jnp.int32, (nblk, tok), 0)
        pos = lax.broadcasted_iota(jnp.int32, (1, tok), 1)
        lists = []
        for slot in range(chosen_s.shape[2]):
            ids = jnp.full((1, tok), NO_BLOCK, jnp.int32)
            for b in range(nblk):
                block = chosen_s[b, 0, slot]
                block = jnp.where(block < me * nblk + b, block, NO_BLOCK)
                ids = jnp.where(pos >= b * blk, block, ids)
            lists.append(ids)
        lists.append(me * nblk + pos // blk)
        for o in range(REACH + 1):
            ids = row + (me - o) * nblk
            hit = ids == lists[0]
            for other in lists[1:]:
                hit = hit | (ids == other)
            marked = jnp.where(hit, 0.0, MASKED)
            if o % 2:
                bias_out[o // 2] = marked
            else:
                bias_own[o // 2] = marked
        key_row = lax.broadcasted_iota(jnp.int32, (blk, tok), 0)
        query = lax.broadcasted_iota(jnp.int32, (blk, tok), 1)
        for j in range(nblk):
            own_bias[j * blk : (j + 1) * blk, :] = jnp.where(
                key_row + j * blk > query, MASKED, bias_own[0, j : j + 1, :]
            )
    all_of(do6.at[0], ld_sem.at[6]).wait()
    send_do.start()
    send_bias.start()

    load_x.wait()
    with scope("xT"):
        x_t[...] = x_s[...].T.reshape(x_t.shape)

    def end_rows(t):
        return pl.ds(lax.rem(t, 2) * half, half)

    early = end_rows(tp)
    x_copies = []
    for dt in range(1, nt):
        other = lax.rem(tp + dt, nt)
        for s in range(2):
            par = 1 - s
            kv = me + par - core
            x_copies.append(
                remote(
                    x_t.at[early, par],
                    x_in.at[tp, core, early],
                    x_send.at[dt - 1],
                    x_recv.at[nt - dt - 1],
                    kv,
                    other,
                )
            )
    for copy in x_copies:
        copy.start()

    zero = jnp.zeros((tok, hd), bf)
    for d in range(1, SPAN):

        @pl.when(chip < d)
        def _():
            kw[d] = zero
            vw[d] = zero

        @pl.when(chip + d >= chips)
        def _():
            dvi[d - 1] = zero

    @pl.when(side == 1)
    def _():
        dki[0] = zero

    @pl.when(ahead < 2)
    def _():
        dki[1] = zero

    def weights(whose, slot, d, bias, buf):
        keys = kw[d]
        for a in range(heads):
            s = lax.dot_general(keys, q6[whose, a], NT, preferred_element_type=f32)
            s = s * (scale * LOG2E)
            lse = lse_s[whose, a : a + 1, :] * LOG2E
            if bias is None:
                p = jnp.exp2(s + (own_bias[...] - lse))
            else:
                p = jnp.exp2(s.reshape(nblk, blk, tok) + (bias - lse)[:, None, :]).reshape(tok, tok)
            p_s[a, slot] = p
            pb_s[buf, :, a * tok : (a + 1) * tok] = p.astype(bf)
        return jnp.dot(
            pb_s[buf], do6[whose].reshape(heads * tok, hd), preferred_element_type=f32
        )

    near = 1 - core
    far = 2 * core

    def far_tile():
        dv_far[...] = weights(1, SPAN + 1, far, bias_sib[core], 0)

    with scope("tile0"):
        dv_own[...] = weights(0, 0, 0, None, 0)

    with scope("q_wait"):
        all_of(q6, sib_recv.at[0]).wait()
        send_lse.wait_recv()
        send_bias.wait_recv()

    relay(1)

    @pl.when(core == 0)
    def _():
        with scope("far0"):
            far_tile()

    def tile1():
        with scope("k1_wait"):

            @pl.when(chip >= 1)
            def _():
                k_copy(1).wait_recv()

        with scope("d1"):
            dvo[0] = (
                weights(0, 1, 1, bias_own[1], 1) + weights(1, SPAN, 1, bias_sib[near], 0)
            ).astype(bf)

        @pl.when(chip >= 1)
        def _():
            dv_copy(1).start()

    def tile2():
        with scope("k2_wait"):

            @pl.when(chip >= 2)
            def _():
                k_copy(2).wait_recv()

        @pl.when(core == 1)
        def _():
            with scope("far1"):
                far_tile()

        with scope("d2"):
            dvo[1] = (
                weights(0, 2, 2, bias_own[2], 1) + jnp.where(core == 1, dv_far[...], 0.0)
            ).astype(bf)

        @pl.when(chip >= 2)
        def _():
            dv_copy(2).start()

    @pl.when(side == 0)
    def _():
        tile2()
        tile1()

    @pl.when(side == 1)
    def _():
        tile1()
        tile2()

    send_x.start()
    relay(2)
    for d in range(SPAN):
        kt[d] = kw[d].T

    with scope("v_wait"):
        each_count(behind, lambda rows: all_of(vw.at[rows], v_recv).wait())

    with scope("sib_gw"):
        for a in range(heads):
            total = jnp.zeros((1, tok), f32)
            for i, d in enumerate((1, far)):
                gw = lax.dot_general(vw[d], do6[1, a], NT, preferred_element_type=f32)
                t = p_s[a, SPAN + i] * gw
                t_s[a, i] = t
                total = total + jnp.sum(t, 0, keepdims=True)
            dl_out[a : a + 1, :] = total
    send_dl.start()

    with scope("dv_wait"):
        each_count(ahead, lambda rows: all_of(dvi.at[rows], dv_recv).wait())

    value = dv_own[...] + jnp.where(core == 0, dv_far[...], 0.0)
    for d in range(1, SPAN):
        value = value + dvi[d - 1].astype(f32)
    value = value.astype(bf)
    vg_ref[...] = value
    vall[tp * 2 + core] = value
    my_vg = vall.at[tp * 2 + core]
    vg_copies = [remote(my_vg, my_vg, vg_send, vg_recv.at[tp * 2 + core], sib)]
    for dt in range(1, nt):
        vg_copies.append(
            remote(my_vg, my_vg, vg_send, vg_recv.at[tp * 2 + core], me, lax.rem(tp + dt, nt))
        )
    for copy in vg_copies:
        copy.start()

    def score_grad(a):
        gw = lax.dot_general(
            vw[...].reshape(SPAN * tok, hd), do6[0, a], NT, preferred_element_type=f32
        )
        p = p_s[a, :SPAN].reshape(SPAN * tok, tok)
        own = jnp.sum(p * gw, 0, keepdims=True)
        dt_out[a : a + 1, :] = own
        delta = own + dl_in[a : a + 1, :]
        ds_own[:, a * tok : (a + 1) * tok] = (p * (gw - delta)).astype(bf)

    with scope("dl_wait"):
        send_dl.wait_recv()
    split = heads // 2
    with scope("own_ds_a"):
        for a in range(split):
            score_grad(a)

    def rs_copy(m):
        return remote(zo.at[m], ri.at[mine], rs_send, rs_recv, (2 * m + side) * 2 + core)

    def vg_wait(t, c):
        all_of(vall.at[t * 2 + c], vg_recv.at[t * 2 + c]).wait()

    def y_copy(g, first):
        rows = pl.ds(first // 2, hh)
        return remote(po.at[rows, 1 - side], yi.at[rows], y_send, y_recv.at[g], across)

    def put_rows(g, first, part):
        rows = pl.ds(first // 2, hh)
        pf[rows] = part.reshape(hh, 2, rw, hd)
        po[rows] = part.astype(bf).reshape(hh, 2, rw, hd)
        y_copy(g, first).start()

    def pass_rows(first):
        @pl.loop(0, hh)
        def _(j):
            @pl.when(first // 2 + j != mine)
            def _():
                rs_copy(first // 2 + j).start()

    def join_rows(g, first):
        with scope(f"y_wait{g}"):
            y_copy(g, first).wait_recv()
        rows = pl.ds(first // 2, hh)
        zo[rows] = (pf[rows, side] + yi[rows].astype(f32)).astype(bf)
        pass_rows(first)

    with scope("vg_wait"):
        vg_wait(tp, 1 - core)
        send_x.wait_recv()

    def own_rows(first, t):
        rows = pl.ds(first, half)
        return jnp.dot(
            x_t[rows, core].reshape(half * rw, tok), vall[t * 2 + core], preferred_element_type=f32
        ) + jnp.dot(
            x_in[tp, 1 - core, rows].reshape(half * rw, tok),
            vall[t * 2 + 1 - core],
            preferred_element_type=f32,
        )

    with scope("relay"):
        relay(LAST)
    groups = []
    with scope("w_end"):
        first = tp * per_tp + (1 - mid) * half
        put_rows(0, first, own_rows((1 - mid) * half, tp))
        groups.append((0, first))
    with scope("w_mid"):
        first = tp * per_tp + mid * half
        put_rows(nt, first, own_rows(mid * half, tp))
        groups.append((nt, first))

    with scope("own_ds_b"):
        for a in range(split, heads):
            score_grad(a)
    send_dt.start()

    def dk_part(ds, d, whose):
        return jnp.dot(
            ds[d * tok : (d + 1) * tok, :],
            q6[whose].reshape(heads * tok, hd),
            preferred_element_type=f32,
        )

    with scope("dk_own"):
        for d in range(1, SPAN):
            dk_acc[d - 1] = dk_part(ds_own, d, 0)

    for dt in range(1, nt):
        t = lax.rem(tp + dt, nt)
        rows = end_rows(t)
        with scope("x_wait"):
            all_of(x_in.at[t, :, rows], x_recv.at[dt - 1]).wait()
        with scope("w_early"):
            part = sum(
                jnp.dot(
                    x_in[t, c, rows].reshape(half * rw, tok),
                    vall[tp * 2 + c],
                    preferred_element_type=f32,
                )
                for c in range(2)
            )
            first = t * per_tp + lax.rem(t, 2) * half
            put_rows(dt, first, part)
            groups.append((dt, first))

    for dt in range(1, nt):
        i = lax.rem(tp + dt, nt) * 2 + core
        with scope("vg_x_wait"):
            all_of(vall.at[i], vg_recv.at[i]).wait()
        remote(vall.at[i], vall.at[i], vg_send, vg_recv.at[i], sib).start()

    with scope("dt_wait"):
        send_dt.wait_recv()
    with scope("sib_ds"):
        for a in range(heads):
            delta = dl_out[a : a + 1, :] + dt_in[a : a + 1, :]
            for i in range(2):
                ds_sib[i * tok : (i + 1) * tok, a * tok : (a + 1) * tok] = (
                    t_s[a, i] - p_s[a, SPAN + i] * delta
                ).astype(bf)
    with scope("dk_sib"):
        dko[0] = ((dk_acc[0] + dk_part(ds_sib, 0, 1)) * scale).astype(bf)
        dk_far = dk_part(ds_sib, 1, 1)
        dk_far2[...] = (dk_acc[1] + jnp.where(core == 1, dk_far, 0.0)) * scale
        dk_acc[0] = jnp.where(core == 0, dk_far, 0.0)
    merge = (side == 1) & (chip >= 3)
    hand = remote(dko.at[0], dk_pass, back_send, pass_recv, across)

    @pl.when(side == 1)
    def _():
        dk_copy(1).start()

    @pl.when((side == 0) & (chip >= 2))
    def _():
        hand.start()
        dko[1] = dk_far2[...].astype(bf)
        dk_copy(2).start()

    def merge_key():
        @pl.when(merge)
        def _():
            with scope("pass_wait"):
                hand.wait_recv()
            dko[1] = (dk_far2[...] + dk_pass[...].astype(f32)).astype(bf)
            dk_copy(2).start()

    def late_copy(dt, i):
        return remote(
            late.at[dt - 1, :, side if i == 0 else 1 - side],
            late_in.at[tp, side],
            late_send,
            late_recv.at[nt - dt - 1],
            me if i == 0 else across,
            lax.rem(tp + dt, nt),
        )

    pl.semaphore_wait(go_sem.at[2], nt - 1)
    for dt in range(1, nt):
        t = lax.rem(tp + dt, nt)
        with scope("vg_other_wait"):
            vg_wait(t, 1 - core)
        with scope("w_late"):
            late[dt - 1] = own_rows(mid * half, t).astype(bf).reshape(hh, 2, rw, hd)
            for i in (1, 0):
                late_copy(dt, i).start()

    def join_late():
        for dt in range(1, nt):
            t = lax.rem(tp + dt, nt)
            first = t * per_tp + (1 - lax.rem(t, 2)) * half
            with scope("late_wait"):
                all_of(late_in.at[t], late_recv.at[dt - 1]).wait()
            zo[pl.ds(first // 2, hh)] = (
                late_in[t, 0].astype(f32) + late_in[t, 1].astype(f32)
            ).astype(bf)
            pass_rows(first)

    def query_sib(i):
        with scope("dq_sib"):
            for a in range(i * split, (i + 1) * split):
                cols = pl.ds(a * tok, tok)
                dq = jnp.dot(kt[1], ds_sib[:tok, cols], preferred_element_type=f32) + jnp.dot(
                    kt[far], ds_sib[tok:, cols], preferred_element_type=f32
                )
                dq_out[a] = (dq * scale).astype(bf)
        send_dq[i].start()

    join_rows(*groups[0])
    query_sib(0)
    for group in groups[2:]:
        join_rows(*group)
    join_rows(*groups[1])
    query_sib(1)
    with scope("dk0"):
        key = (dk_acc[0] + dk_part(ds_own, 0, 0)) * scale
    merge_key()
    join_late()

    with scope("dq_own"):
        for i in range(2):
            send_dq[i].wait_recv()
            for a in range(i * split, (i + 1) * split):
                dq = sum(
                    jnp.dot(
                        kt[d],
                        ds_own[d * tok : (d + 1) * tok, a * tok : (a + 1) * tok],
                        preferred_element_type=f32,
                    )
                    for d in range(SPAN)
                )
                dq = dq * scale + dq_in[a].astype(f32)
                qg_ref[:, a * hd : (a + 1) * hd] = dq.T.astype(bf)

    with scope("dk_wait"):

        @pl.when((side == 0) & (ahead >= 2))
        def _():
            all_of(dki, dk_recv).wait()

        @pl.when((side == 0) != (ahead >= 2))
        def _():
            all_of(dki.at[0], dk_recv).wait()

    for d in range(BACK):
        key = key + dki[d].astype(f32)
    kg_ref[...] = key.astype(bf)

    with scope("rs_wait"):

        ri[pl.ds(mine, 1)] = zo[pl.ds(mine, 1)]
        all_of(ri.at[pl.ds(0, pairs - 1)], rs_recv).wait()
    wg_ref[...] = jnp.sum(ri[...].astype(f32), 0)

    with scope("send_wait"):
        each_count(ahead, lambda rows: all_of(kvw.at[:, rows], kv_send).wait())
        each_count(behind, lambda rows: all_of(back_out.at[:, rows], back_send).wait())
        all_of(q6, sib_send.at[0]).wait()
        send_lse.wait_send()
        send_bias.wait_send()
        send_x.wait_send()
        all_of(lse_s, sib_send.at[4]).wait()
        all_of(dq_out, sib_send.at[5]).wait()
        for dt in range(1, nt):
            all_of(x_t.at[early], x_send.at[dt - 1]).wait()
        all_of(vall.at[pl.ds(0, 2 * nt - 1)], vg_send).wait()
        all_of(late, late_send).wait()
        all_of(po.at[pl.ds(0, (nt + 1) * hh), 0], y_send).wait()
        all_of(ri.at[pl.ds(0, pairs - 1)], rs_send).wait()


def finish(*refs):
    count = len(refs) // 2
    sems = refs[-1]
    copies = [
        pltpu.make_async_copy(refs[i], refs[count + i], sems.at[i]) for i in range(count)
    ]
    for copy in copies:
        copy.start()
    for copy in copies:
        copy.wait()


def shards(nk, nt, queries, keys, values, log_sums, out_grad, chosen, inputs):
    tok, hd = keys.shape
    heads = queries.shape[1] // hd
    nblk = chosen.shape[0]
    feats = inputs.shape[1]
    rw = feats * nt // nk
    per_tp = feats // (2 * rw)
    bf, f32 = jnp.bfloat16, jnp.float32
    dma = pltpu.SemaphoreType.DMA
    vmem = pl.BlockSpec(memory_space=pltpu.VMEM)
    hbm = pl.BlockSpec(memory_space=pltpu.HBM)
    pairs = nk // 4
    parts = pl.pallas_call(
        functools.partial(kernel, nk, nt),
        out_shape=(
            pltpu.VMEM((tok, heads * hd), bf),
            pltpu.VMEM((tok, hd), bf),
            pltpu.VMEM((tok, hd), bf),
            pltpu.VMEM((rw, hd), f32),
        ),
        in_specs=[hbm] * 7,
        out_specs=(vmem, vmem, vmem, vmem),
        scratch_shapes=[
            pltpu.SMEM(chosen.shape, jnp.int32),
            pltpu.VMEM((2, heads, tok), f32),
            pltpu.VMEM((2, heads, tok, hd), bf),
            pltpu.VMEM((2, heads, tok, hd), bf),
            pltpu.VMEM((tok, feats), bf),
            pltpu.VMEM((2, SPAN, tok, hd), bf),
            pltpu.VMEM((SPAN, hd, tok), bf),
            pltpu.VMEM((SPAN, nblk, tok), f32),
            pltpu.VMEM((2, nblk, tok), f32),
            pltpu.VMEM((2, nblk, tok), f32),
            pltpu.VMEM((tok, tok), f32),
            pltpu.VMEM((heads, SPAN + 2, tok, tok), f32),
            pltpu.VMEM((heads, 2, tok, tok), f32),
            pltpu.VMEM((2, tok, heads * tok), bf),
            pltpu.VMEM((SPAN * tok, heads * tok), bf),
            pltpu.VMEM((2 * tok, heads * tok), bf),
            pltpu.VMEM((tok, hd), f32),
            pltpu.VMEM((tok, hd), f32),
            pltpu.VMEM((BACK, tok, hd), f32),
            pltpu.VMEM((2, BACK, tok, hd), bf),
            pltpu.VMEM((2, BACK, tok, hd), bf),
            pltpu.VMEM((tok, hd), bf),
            pltpu.VMEM((tok, hd), f32),
            pltpu.VMEM((heads, tok), f32),
            pltpu.VMEM((heads, tok), f32),
            pltpu.VMEM((heads, tok), f32),
            pltpu.VMEM((heads, tok), f32),
            pltpu.VMEM((heads, hd, tok), bf),
            pltpu.VMEM((heads, hd, tok), bf),
            pltpu.VMEM((per_tp, 2, rw, tok), bf),
            pltpu.VMEM((nt, 2, per_tp, rw, tok), bf),
            pltpu.VMEM((2 * nt, tok, hd), bf),
            pltpu.VMEM((nt - 1, per_tp // 4, 2, rw, hd), bf),
            pltpu.VMEM((nt, 2, per_tp // 4, rw, hd), bf),
            pltpu.VMEM((pairs, 2, rw, hd), f32),
            pltpu.VMEM((pairs, 2, rw, hd), bf),
            pltpu.VMEM((pairs, rw, hd), bf),
            pltpu.VMEM((pairs, rw, hd), bf),
            pltpu.VMEM((pairs, rw, hd), bf),
            dma((7,)),
            dma,
            dma((BACK,)),
            dma,
            dma,
            dma,
            dma,
            dma,
            dma((6,)),
            dma((8,)),
            dma((nt - 1,)),
            dma((nt - 1,)),
            dma,
            dma((2 * nt,)),
            dma,
            dma((nt - 1,)),
            dma,
            dma((nt + 1,)),
            dma,
            dma,
            pltpu.SemaphoreType.REGULAR((3,)),
        ],
        compiler_params=pltpu.CompilerParams(
            collective_id=0, has_side_effects=True, vmem_limit_bytes=60 * 1024 * 1024
        ),
    )(chosen, log_sums, keys, values, queries, out_grad, inputs)
    return pl.pallas_call(
        finish,
        out_shape=tuple(jax.ShapeDtypeStruct(part.shape, part.dtype) for part in parts),
        in_specs=[vmem] * len(parts),
        out_specs=(hbm,) * len(parts),
        scratch_shapes=[dma((len(parts),))],
    )(*(pltpu.with_memory_space_constraint(part, pltpu.VMEM) for part in parts))


def solution(mesh):
    in_specs = (
        P("kv", "tp"),
        P("kv", "tp"),
        P("kv", "tp"),
        P("tp", "kv"),
        P("kv", "tp"),
        P("kv", "tp", None),
        P("kv", "tp"),
    )
    out_specs = (P("kv", "tp"), P("kv", "tp"), P("kv", "tp"), P("kv", "tp"))
    return jax.shard_map(
        functools.partial(shards, mesh.shape["kv"], mesh.shape["tp"]),
        mesh=mesh,
        in_specs=in_specs,
        out_specs=out_specs,
        check_vma=False,
    )
```

```python
import functools

import jax
import jax.numpy as jnp
from jax import lax
from jax.experimental import pallas as pl
from jax.experimental.pallas import tpu as pltpu
from jax.sharding import PartitionSpec as P

REACH = 4
BACK = REACH // 2
SPAN = BACK + 1
STEPS = tuple(step for d in range(1, BACK + 1) for step in (d, -d))
LAST = 3
MASKED = -1e30
NO_BLOCK = -(1 << 20)
LOG2E = 1.4426950408889634
MESH = pl.DeviceIdType.MESH
NT = (((1,), (1,)), ((), ()))
scope = jax.named_scope


def kernel(
    nk,
    nt,
    chosen_hbm,
    lse_hbm,
    k_hbm,
    v_hbm,
    q_hbm,
    do_hbm,
    x_hbm,
    qg_ref,
    kg_ref,
    vg_ref,
    wg_ref,
    chosen_s,
    lse_s,
    q6,
    do6,
    x_s,
    kvw,
    kt,
    bias_own,
    bias_out,
    bias_sib,
    own_bias,
    p_s,
    t_s,
    pb_s,
    ds_own,
    ds_sib,
    dv_own,
    dv_far,
    dk_acc,
    back_out,
    back_in,
    dk_pass,
    dk_far2,
    dl_out,
    dl_in,
    dt_out,
    dt_in,
    dq_out,
    dq_in,
    x_t,
    x_in,
    vall,
    late,
    late_in,
    pf,
    po,
    yi,
    zo,
    ri,
    ld_sem,
    k_recv,
    v_recv,
    dv_recv,
    dk_recv,
    pass_recv,
    sib_send,
    sib_recv,
    x_send,
    x_recv,
    vg_send,
    vg_recv,
    late_send,
    late_recv,
    y_send,
    y_recv,
    rs_send,
    rs_recv,
    go_sem,
):
    me = lax.axis_index("kv")
    tp = lax.axis_index("tp")
    core = lax.rem(me, 2)
    chip = me // 2
    sib = me + 1 - 2 * core
    side = lax.rem(chip, 2)
    across = me + 2 - 4 * side
    chips = nk // 2
    _, heads, tok, hd = q6.shape
    kw, vw = kvw.at[0], kvw.at[1]
    dvo, dko = back_out.at[0], back_out.at[1]
    dvi, dki = back_in.at[0], back_in.at[1]
    nblk = chosen_s.shape[0]
    blk = tok // nblk
    scale = hd**-0.5
    per_tp, _, rw, _ = x_t.shape
    half = per_tp // 2
    pairs = chips // 2
    hh = half // 2
    mine = chip // 2
    half_heads = heads // 2
    mid = 1 - lax.rem(tp, 2)
    f32, bf = jnp.float32, jnp.bfloat16

    behind = chip
    ahead = chips - 1 - chip
    near_chips = [(step, ahead >= step if step > 0 else behind >= -step) for step in STEPS]
    kv_send, back_send = ld_sem.at[0], ld_sem.at[1]
    sib_sends = [ld_sem.at[i] for i in (5, 4, 3, 6)] + [sib_send.at[0], sib_send.at[1]]
    barrier = pltpu.get_barrier_semaphore()
    count = 1 + 2 * (nt - 1)
    for step, exists in near_chips:
        count = count + jnp.where(exists, 1, 0)

        @pl.when(exists)
        def _():
            pl.semaphore_signal(
                barrier, inc=1, device_id=(me + 2 * step, tp), device_id_type=MESH
            )

    pl.semaphore_signal(barrier, inc=1, device_id=(sib, tp), device_id_type=MESH)
    for dt in range(1, nt):
        for kv in (me, sib):
            pl.semaphore_signal(
                barrier, inc=1, device_id=(kv, lax.rem(tp + dt, nt)), device_id_type=MESH
            )

    load_k, load_v, load_x, load_chosen, load_lse = (
        pltpu.make_async_copy(src, dst, ld_sem.at[i])
        for i, (src, dst) in enumerate(
            (
                (k_hbm, kw.at[0]),
                (v_hbm, vw.at[0]),
                (x_hbm, x_s),
                (chosen_hbm, chosen_s),
                (lse_hbm, lse_s.at[0]),
            )
        )
    )
    load_q, load_do = (
        [
            pltpu.make_async_copy(src.at[:, pl.ds(a * hd, hd)], dst.at[0, a], ld_sem.at[i])
            for a in range(heads)
        ]
        for i, src, dst in ((5, q_hbm, q6), (6, do_hbm, do6))
    )

    def all_of(ref, sem):
        return pltpu.make_async_copy(ref, ref, sem)

    for load in (load_k, load_chosen, *load_q, load_lse, load_v, *load_do, load_x):
        load.start()

    def remote(src, dst, send, recv, kv, t=None):
        return pltpu.make_async_remote_copy(
            src_ref=src,
            dst_ref=dst,
            send_sem=send,
            recv_sem=recv,
            device_id=(kv, tp if t is None else t),
            device_id_type=MESH,
        )

    def k_copy(d):
        return remote(kw.at[0], kw.at[d], kv_send, k_recv.at[d - 1], me + 2 * d)

    def v_copy(d):
        return remote(vw.at[0], vw.at[d], kv_send, v_recv, me + 2 * d)

    def dv_copy(d):
        return remote(dvo.at[d - 1], dvi.at[d - 1], back_send, dv_recv, me - 2 * d)

    def dk_copy(d):
        return remote(dko.at[d - 1], dki.at[d - 1], back_send, dk_recv, me - 2 * d)

    def each_count(left, wait):
        for count in range(1, BACK + 1):
            here = (left == count) if count < BACK else (left >= count)

            @pl.when(here)
            def _():
                wait(pl.ds(0, count))

    def to_sib(i, j, src, dst):
        return remote(src, dst, sib_sends[i], sib_recv.at[j], sib)

    send_q = to_sib(0, 0, q6.at[0], q6.at[1])
    send_do = to_sib(0, 0, do6.at[0], do6.at[1])
    send_lse = to_sib(1, 1, lse_s.at[0], lse_s.at[1])
    send_bias = to_sib(2, 2, bias_out, bias_sib)
    send_x = to_sib(3, 3, x_t.at[:, 1 - core], x_in.at[tp, core])
    send_dl = to_sib(4, 4, dl_out, dl_in)
    send_dt = to_sib(4, 5, dt_out, dt_in)
    send_dq = [
        to_sib(5, 6 + i, dq_out.at[pl.ds(i * half_heads, half_heads)], dq_in.at[pl.ds(i * half_heads, half_heads)])
        for i in range(2)
    ]

    with scope("barrier_wait"):
        pl.semaphore_wait(barrier, count)
    for dt in range(1, nt):
        pl.semaphore_signal(
            go_sem.at[2], inc=1, device_id=(me, lax.rem(tp + dt, nt)), device_id_type=MESH
        )

    def relay(point):
        for i, step, left, done in ((0, -BACK, ahead, behind), (1, BACK, behind, ahead)):
            hops = left // BACK
            turn = hops == point if point < LAST else hops >= point

            @pl.when(turn & (hops > 0))
            def _():
                pl.semaphore_wait(go_sem.at[i], 1)

            @pl.when(turn & (done >= BACK))
            def _():
                pl.semaphore_signal(
                    go_sem.at[i], inc=1, device_id=(me + 2 * step, tp), device_id_type=MESH
                )

    load_k.wait()
    for d in range(1, SPAN):

        @pl.when(chip + d < chips)
        def _():
            k_copy(d).start()

    relay(0)
    all_of(q6.at[0], ld_sem.at[5]).wait()
    send_q.start()
    load_lse.wait()
    send_lse.start()
    load_v.wait()
    for d in range(1, SPAN):

        @pl.when(chip + d < chips)
        def _():
            v_copy(d).start()

    load_chosen.wait()
    with scope("bias"):
        row = lax.broadcasted_iota(jnp.int32, (nblk, tok), 0)
        pos = lax.broadcasted_iota(jnp.int32, (1, tok), 1)
        lists = []
        for slot in range(chosen_s.shape[2]):
            ids = jnp.full((1, tok), NO_BLOCK, jnp.int32)
            for b in range(nblk):
                block = chosen_s[b, 0, slot]
                block = jnp.where(block < me * nblk + b, block, NO_BLOCK)
                ids = jnp.where(pos >= b * blk, block, ids)
            lists.append(ids)
        lists.append(me * nblk + pos // blk)
        for o in range(REACH + 1):
            ids = row + (me - o) * nblk
            hit = ids == lists[0]
            for other in lists[1:]:
                hit = hit | (ids == other)
            marked = jnp.where(hit, 0.0, MASKED)
            if o % 2:
                bias_out[o // 2] = marked
            else:
                bias_own[o // 2] = marked
        key_row = lax.broadcasted_iota(jnp.int32, (blk, tok), 0)
        query = lax.broadcasted_iota(jnp.int32, (blk, tok), 1)
        for j in range(nblk):
            own_bias[j * blk : (j + 1) * blk, :] = jnp.where(
                key_row + j * blk > query, MASKED, bias_own[0, j : j + 1, :]
            )
    all_of(do6.at[0], ld_sem.at[6]).wait()
    send_do.start()
    send_bias.start()

    load_x.wait()
    with scope("xT"):
        x_t[...] = x_s[...].T.reshape(x_t.shape)

    def end_rows(t):
        return pl.ds(lax.rem(t, 2) * half, half)

    early = end_rows(tp)
    x_copies = []
    for dt in range(1, nt):
        other = lax.rem(tp + dt, nt)
        for s in range(2):
            par = 1 - s
            kv = me + par - core
            x_copies.append(
                remote(
                    x_t.at[early, par],
                    x_in.at[tp, core, early],
                    x_send.at[dt - 1],
                    x_recv.at[nt - dt - 1],
                    kv,
                    other,
                )
            )
    for copy in x_copies:
        copy.start()

    zero = jnp.zeros((tok, hd), bf)
    for d in range(1, SPAN):

        @pl.when(chip < d)
        def _():
            kw[d] = zero
            vw[d] = zero

        @pl.when(chip + d >= chips)
        def _():
            dvi[d - 1] = zero

    @pl.when(side == 1)
    def _():
        dki[0] = zero

    @pl.when(ahead < 2)
    def _():
        dki[1] = zero

    def weights(whose, slot, d, bias, buf):
        keys = kw[d]
        for a in range(heads):
            s = lax.dot_general(keys, q6[whose, a], NT, preferred_element_type=f32)
            s = s * (scale * LOG2E)
            lse = lse_s[whose, a : a + 1, :] * LOG2E
            if bias is None:
                p = jnp.exp2(s + (own_bias[...] - lse))
            else:
                p = jnp.exp2(s.reshape(nblk, blk, tok) + (bias - lse)[:, None, :]).reshape(tok, tok)
            p_s[a, slot] = p
            pb_s[buf, :, a * tok : (a + 1) * tok] = p.astype(bf)
        return jnp.dot(
            pb_s[buf], do6[whose].reshape(heads * tok, hd), preferred_element_type=f32
        )

    near = 1 - core
    far = 2 * core

    def far_tile():
        dv_far[...] = weights(1, SPAN + 1, far, bias_sib[core], 0)

    with scope("tile0"):
        dv_own[...] = weights(0, 0, 0, None, 0)

    with scope("q_wait"):
        all_of(q6, sib_recv.at[0]).wait()
        send_lse.wait_recv()
        send_bias.wait_recv()

    relay(1)

    @pl.when(core == 0)
    def _():
        with scope("far0"):
            far_tile()

    def tile1():
        with scope("k1_wait"):

            @pl.when(chip >= 1)
            def _():
                k_copy(1).wait_recv()

        with scope("d1"):
            dvo[0] = (
                weights(0, 1, 1, bias_own[1], 1) + weights(1, SPAN, 1, bias_sib[near], 0)
            ).astype(bf)

        @pl.when(chip >= 1)
        def _():
            dv_copy(1).start()

    def tile2():
        with scope("k2_wait"):

            @pl.when(chip >= 2)
            def _():
                k_copy(2).wait_recv()

        @pl.when(core == 1)
        def _():
            with scope("far1"):
                far_tile()

        with scope("d2"):
            dvo[1] = (
                weights(0, 2, 2, bias_own[2], 1) + jnp.where(core == 1, dv_far[...], 0.0)
            ).astype(bf)

        @pl.when(chip >= 2)
        def _():
            dv_copy(2).start()

    @pl.when(side == 0)
    def _():
        tile2()
        tile1()

    @pl.when(side == 1)
    def _():
        tile1()
        tile2()

    send_x.start()
    relay(2)
    for d in range(SPAN):
        kt[d] = kw[d].T

    with scope("v_wait"):
        each_count(behind, lambda rows: all_of(vw.at[rows], v_recv).wait())

    with scope("sib_gw"):
        for a in range(heads):
            total = jnp.zeros((1, tok), f32)
            for i, d in enumerate((1, far)):
                gw = lax.dot_general(vw[d], do6[1, a], NT, preferred_element_type=f32)
                t = p_s[a, SPAN + i] * gw
                t_s[a, i] = t
                total = total + jnp.sum(t, 0, keepdims=True)
            dl_out[a : a + 1, :] = total
    send_dl.start()

    with scope("dv_wait"):
        each_count(ahead, lambda rows: all_of(dvi.at[rows], dv_recv).wait())

    value = dv_own[...] + jnp.where(core == 0, dv_far[...], 0.0)
    for d in range(1, SPAN):
        value = value + dvi[d - 1].astype(f32)
    value = value.astype(bf)
    vg_ref[...] = value
    vall[tp * 2 + core] = value
    my_vg = vall.at[tp * 2 + core]
    vg_copies = [remote(my_vg, my_vg, vg_send, vg_recv.at[tp * 2 + core], sib)]
    for dt in range(1, nt):
        vg_copies.append(
            remote(my_vg, my_vg, vg_send, vg_recv.at[tp * 2 + core], me, lax.rem(tp + dt, nt))
        )
    for copy in vg_copies:
        copy.start()

    def score_grad(a):
        gw = lax.dot_general(
            vw[...].reshape(SPAN * tok, hd), do6[0, a], NT, preferred_element_type=f32
        )
        p = p_s[a, :SPAN].reshape(SPAN * tok, tok)
        own = jnp.sum(p * gw, 0, keepdims=True)
        dt_out[a : a + 1, :] = own
        delta = own + dl_in[a : a + 1, :]
        ds_own[:, a * tok : (a + 1) * tok] = (p * (gw - delta)).astype(bf)

    with scope("dl_wait"):
        send_dl.wait_recv()
    split = heads // 2
    with scope("own_ds_a"):
        for a in range(split):
            score_grad(a)

    def rs_copy(m):
        return remote(zo.at[m], ri.at[mine], rs_send, rs_recv, (2 * m + side) * 2 + core)

    def vg_wait(t, c):
        all_of(vall.at[t * 2 + c], vg_recv.at[t * 2 + c]).wait()

    def y_copy(g, first):
        rows = pl.ds(first // 2, hh)
        return remote(po.at[rows, 1 - side], yi.at[rows], y_send, y_recv.at[g], across)

    def put_rows(g, first, part):
        rows = pl.ds(first // 2, hh)
        pf[rows] = part.reshape(hh, 2, rw, hd)
        po[rows] = part.astype(bf).reshape(hh, 2, rw, hd)
        y_copy(g, first).start()

    def pass_rows(first):
        @pl.loop(0, hh)
        def _(j):
            @pl.when(first // 2 + j != mine)
            def _():
                rs_copy(first // 2 + j).start()

    def join_rows(g, first):
        with scope(f"y_wait{g}"):
            y_copy(g, first).wait_recv()
        rows = pl.ds(first // 2, hh)
        zo[rows] = (pf[rows, side] + yi[rows].astype(f32)).astype(bf)
        pass_rows(first)

    with scope("vg_wait"):
        vg_wait(tp, 1 - core)
        send_x.wait_recv()

    def own_rows(first, t):
        rows = pl.ds(first, half)
        return jnp.dot(
            x_t[rows, core].reshape(half * rw, tok), vall[t * 2 + core], preferred_element_type=f32
        ) + jnp.dot(
            x_in[tp, 1 - core, rows].reshape(half * rw, tok),
            vall[t * 2 + 1 - core],
            preferred_element_type=f32,
        )

    with scope("relay"):
        relay(LAST)
    groups = []
    with scope("w_end"):
        first = tp * per_tp + (1 - mid) * half
        put_rows(0, first, own_rows((1 - mid) * half, tp))
        groups.append((0, first))
    with scope("w_mid"):
        first = tp * per_tp + mid * half
        put_rows(nt, first, own_rows(mid * half, tp))
        groups.append((nt, first))

    with scope("own_ds_b"):
        for a in range(split, heads):
            score_grad(a)
    send_dt.start()

    def dk_part(ds, d, whose):
        return jnp.dot(
            ds[d * tok : (d + 1) * tok, :],
            q6[whose].reshape(heads * tok, hd),
            preferred_element_type=f32,
        )

    with scope("dk_own"):
        for d in range(1, SPAN):
            dk_acc[d - 1] = dk_part(ds_own, d, 0)

    for dt in range(1, nt):
        t = lax.rem(tp + dt, nt)
        rows = end_rows(t)
        with scope("x_wait"):
            all_of(x_in.at[t, :, rows], x_recv.at[dt - 1]).wait()
        with scope("w_early"):
            part = sum(
                jnp.dot(
                    x_in[t, c, rows].reshape(half * rw, tok),
                    vall[tp * 2 + c],
                    preferred_element_type=f32,
                )
                for c in range(2)
            )
            first = t * per_tp + lax.rem(t, 2) * half
            put_rows(dt, first, part)
            groups.append((dt, first))

    for dt in range(1, nt):
        i = lax.rem(tp + dt, nt) * 2 + core
        with scope("vg_x_wait"):
            all_of(vall.at[i], vg_recv.at[i]).wait()
        remote(vall.at[i], vall.at[i], vg_send, vg_recv.at[i], sib).start()

    with scope("dt_wait"):
        send_dt.wait_recv()
    with scope("sib_ds"):
        for a in range(heads):
            delta = dl_out[a : a + 1, :] + dt_in[a : a + 1, :]
            for i in range(2):
                ds_sib[i * tok : (i + 1) * tok, a * tok : (a + 1) * tok] = (
                    t_s[a, i] - p_s[a, SPAN + i] * delta
                ).astype(bf)
    with scope("dk_sib"):
        dko[0] = ((dk_acc[0] + dk_part(ds_sib, 0, 1)) * scale).astype(bf)
        dk_far = dk_part(ds_sib, 1, 1)
        dk_far2[...] = (dk_acc[1] + jnp.where(core == 1, dk_far, 0.0)) * scale
        dk_acc[0] = jnp.where(core == 0, dk_far, 0.0)
    merge = (side == 1) & (chip >= 3)
    hand = remote(dko.at[0], dk_pass, back_send, pass_recv, across)

    @pl.when(side == 1)
    def _():
        dk_copy(1).start()

    @pl.when((side == 0) & (chip >= 2))
    def _():
        hand.start()
        dko[1] = dk_far2[...].astype(bf)
        dk_copy(2).start()

    def merge_key():
        @pl.when(merge)
        def _():
            with scope("pass_wait"):
                hand.wait_recv()
            dko[1] = (dk_far2[...] + dk_pass[...].astype(f32)).astype(bf)
            dk_copy(2).start()

    if hh % 2 == 0:
        chunks = [(c * hh // 2, hh // 2, pl.ds(0, rw)) for c in range(2)]
    else:
        chunks = [(0, hh, pl.ds(c * rw // 2, rw // 2)) for c in range(2)]

    def late_copy(dt, c, i):
        start, count, rows = chunks[c]
        blocks = pl.ds(start, count)
        return remote(
            late.at[dt - 1, blocks, side if i == 0 else 1 - side, rows],
            late_in.at[tp, side, blocks, rows],
            late_send,
            late_recv.at[nt - dt - 1, c],
            me if i == 0 else across,
            lax.rem(tp + dt, nt),
        )

    pl.semaphore_wait(go_sem.at[2], nt - 1)
    for dt in range(1, nt):
        t = lax.rem(tp + dt, nt)
        with scope("vg_other_wait"):
            vg_wait(t, 1 - core)
        with scope("w_late"):
            late[dt - 1] = own_rows(mid * half, t).astype(bf).reshape(hh, 2, rw, hd)
            for c in range(2):
                for i in (1, 0):
                    late_copy(dt, c, i).start()

    def join_late(c):
        start, count, rows = chunks[c]
        blocks = pl.ds(start, count)
        for dt in range(1, nt):
            t = lax.rem(tp + dt, nt)
            first = (t * per_tp + (1 - lax.rem(t, 2)) * half) // 2 + start
            with scope("late_wait"):
                all_of(late_in.at[t, :, blocks, rows], late_recv.at[dt - 1, c]).wait()
            zo[pl.ds(first, count), rows] = (
                late_in[t, 0, blocks, rows].astype(f32) + late_in[t, 1, blocks, rows].astype(f32)
            ).astype(bf)

            @pl.loop(0, count)
            def _(j):
                m = first + j

                @pl.when(m != mine)
                def _():
                    remote(
                        zo.at[m, rows],
                        ri.at[mine, rows],
                        rs_send,
                        rs_recv,
                        (2 * m + side) * 2 + core,
                    ).start()

    def query_sib(i):
        with scope("dq_sib"):
            for a in range(i * split, (i + 1) * split):
                cols = pl.ds(a * tok, tok)
                dq = jnp.dot(kt[1], ds_sib[:tok, cols], preferred_element_type=f32) + jnp.dot(
                    kt[far], ds_sib[tok:, cols], preferred_element_type=f32
                )
                dq_out[a] = (dq * scale).astype(bf)
        send_dq[i].start()

    join_rows(*groups[0])
    query_sib(0)
    for group in groups[2:]:
        join_rows(*group)
    join_rows(*groups[1])
    query_sib(1)
    with scope("dk0"):
        key = (dk_acc[0] + dk_part(ds_own, 0, 0)) * scale
    merge_key()
    for c in range(2):
        join_late(c)

    with scope("dq_own"):
        for i in range(2):
            send_dq[i].wait_recv()
            for a in range(i * split, (i + 1) * split):
                dq = sum(
                    jnp.dot(
                        kt[d],
                        ds_own[d * tok : (d + 1) * tok, a * tok : (a + 1) * tok],
                        preferred_element_type=f32,
                    )
                    for d in range(SPAN)
                )
                dq = dq * scale + dq_in[a].astype(f32)
                qg_ref[:, a * hd : (a + 1) * hd] = dq.T.astype(bf)

    with scope("dk_wait"):

        @pl.when((side == 0) & (ahead >= 2))
        def _():
            all_of(dki, dk_recv).wait()

        @pl.when((side == 0) != (ahead >= 2))
        def _():
            all_of(dki.at[0], dk_recv).wait()

    for d in range(BACK):
        key = key + dki[d].astype(f32)
    kg_ref[...] = key.astype(bf)

    with scope("rs_wait"):

        ri[pl.ds(mine, 1)] = zo[pl.ds(mine, 1)]
        all_of(ri.at[pl.ds(0, pairs - 1)], rs_recv).wait()
    wg_ref[...] = jnp.sum(ri[...].astype(f32), 0)

    with scope("send_wait"):
        each_count(ahead, lambda rows: all_of(kvw.at[:, rows], kv_send).wait())
        each_count(behind, lambda rows: all_of(back_out.at[:, rows], back_send).wait())
        all_of(q6, sib_sends[0]).wait()
        send_lse.wait_send()
        send_bias.wait_send()
        send_x.wait_send()
        all_of(lse_s, sib_sends[4]).wait()
        all_of(dq_out, sib_sends[5]).wait()
        for dt in range(1, nt):
            all_of(x_t.at[early], x_send.at[dt - 1]).wait()
        all_of(vall.at[pl.ds(0, 2 * nt - 1)], vg_send).wait()
        all_of(late, late_send).wait()
        all_of(po.at[pl.ds(0, (nt + 1) * hh), 0], y_send).wait()
        all_of(ri.at[pl.ds(0, pairs - 1)], rs_send).wait()


def finish(*refs):
    count = len(refs) // 2
    sems = refs[-1]
    copies = [
        pltpu.make_async_copy(refs[i], refs[count + i], sems.at[i]) for i in range(count)
    ]
    for copy in copies:
        copy.start()
    for copy in copies:
        copy.wait()


def shards(nk, nt, queries, keys, values, log_sums, out_grad, chosen, inputs):
    tok, hd = keys.shape
    heads = queries.shape[1] // hd
    nblk = chosen.shape[0]
    feats = inputs.shape[1]
    rw = feats * nt // nk
    per_tp = feats // (2 * rw)
    bf, f32 = jnp.bfloat16, jnp.float32
    dma = pltpu.SemaphoreType.DMA
    vmem = pl.BlockSpec(memory_space=pltpu.VMEM)
    hbm = pl.BlockSpec(memory_space=pltpu.HBM)
    pairs = nk // 4
    parts = pl.pallas_call(
        functools.partial(kernel, nk, nt),
        out_shape=(
            pltpu.VMEM((tok, heads * hd), bf),
            pltpu.VMEM((tok, hd), bf),
            pltpu.VMEM((tok, hd), bf),
            pltpu.VMEM((rw, hd), f32),
        ),
        in_specs=[hbm] * 7,
        out_specs=(vmem, vmem, vmem, vmem),
        scratch_shapes=[
            pltpu.SMEM(chosen.shape, jnp.int32),
            pltpu.VMEM((2, heads, tok), f32),
            pltpu.VMEM((2, heads, tok, hd), bf),
            pltpu.VMEM((2, heads, tok, hd), bf),
            pltpu.VMEM((tok, feats), bf),
            pltpu.VMEM((2, SPAN, tok, hd), bf),
            pltpu.VMEM((SPAN, hd, tok), bf),
            pltpu.VMEM((SPAN, nblk, tok), f32),
            pltpu.VMEM((2, nblk, tok), f32),
            pltpu.VMEM((2, nblk, tok), f32),
            pltpu.VMEM((tok, tok), f32),
            pltpu.VMEM((heads, SPAN + 2, tok, tok), f32),
            pltpu.VMEM((heads, 2, tok, tok), f32),
            pltpu.VMEM((2, tok, heads * tok), bf),
            pltpu.VMEM((SPAN * tok, heads * tok), bf),
            pltpu.VMEM((2 * tok, heads * tok), bf),
            pltpu.VMEM((tok, hd), f32),
            pltpu.VMEM((tok, hd), f32),
            pltpu.VMEM((BACK, tok, hd), f32),
            pltpu.VMEM((2, BACK, tok, hd), bf),
            pltpu.VMEM((2, BACK, tok, hd), bf),
            pltpu.VMEM((tok, hd), bf),
            pltpu.VMEM((tok, hd), f32),
            pltpu.VMEM((heads, tok), f32),
            pltpu.VMEM((heads, tok), f32),
            pltpu.VMEM((heads, tok), f32),
            pltpu.VMEM((heads, tok), f32),
            pltpu.VMEM((heads, hd, tok), bf),
            pltpu.VMEM((heads, hd, tok), bf),
            pltpu.VMEM((per_tp, 2, rw, tok), bf),
            pltpu.VMEM((nt, 2, per_tp, rw, tok), bf),
            pltpu.VMEM((2 * nt, tok, hd), bf),
            pltpu.VMEM((nt - 1, per_tp // 4, 2, rw, hd), bf),
            pltpu.VMEM((nt, 2, per_tp // 4, rw, hd), bf),
            pltpu.VMEM((pairs, 2, rw, hd), f32),
            pltpu.VMEM((pairs, 2, rw, hd), bf),
            pltpu.VMEM((pairs, rw, hd), bf),
            pltpu.VMEM((pairs, rw, hd), bf),
            pltpu.VMEM((pairs, rw, hd), bf),
            dma((7,)),
            dma((BACK,)),
            dma,
            dma,
            dma,
            dma,
            dma((2,)),
            dma((8,)),
            dma((nt - 1,)),
            dma((nt - 1,)),
            dma,
            dma((2 * nt,)),
            dma,
            dma((nt - 1, 2)),
            dma,
            dma((nt + 1,)),
            dma,
            dma,
            pltpu.SemaphoreType.REGULAR((3,)),
        ],
        compiler_params=pltpu.CompilerParams(
            collective_id=0, has_side_effects=True, vmem_limit_bytes=60 * 1024 * 1024
        ),
    )(chosen, log_sums, keys, values, queries, out_grad, inputs)
    return pl.pallas_call(
        finish,
        out_shape=tuple(jax.ShapeDtypeStruct(part.shape, part.dtype) for part in parts),
        in_specs=[vmem] * len(parts),
        out_specs=(hbm,) * len(parts),
        scratch_shapes=[dma((len(parts),))],
    )(*(pltpu.with_memory_space_constraint(part, pltpu.VMEM) for part in parts))


def solution(mesh):
    in_specs = (
        P("kv", "tp"),
        P("kv", "tp"),
        P("kv", "tp"),
        P("tp", "kv"),
        P("kv", "tp"),
        P("kv", "tp", None),
        P("kv", "tp"),
    )
    out_specs = (P("kv", "tp"), P("kv", "tp"), P("kv", "tp"), P("kv", "tp"))
    return jax.shard_map(
        functools.partial(shards, mesh.shape["kv"], mesh.shape["tp"]),
        mesh=mesh,
        in_specs=in_specs,
        out_specs=out_specs,
        check_vma=False,
    )
```
